32 devices in a mesh: sp: 8 (over z, y), tp: 4 (over x, core).
Axes of the slice: x: 2, y: 2, z: 4, core: 2. Of those that a mesh axis runs over, the one named last changes fastest.
Arguments:
- queries: bfloat16 [8192, 1024], P('sp', 'tp'), may hold values from -6 to 6
- keys: bfloat16 [8192, 1024], P('sp', 'tp'), may hold values from -6 to 6
- values: bfloat16 [8192, 2048], P('sp', 'tp'), may hold values from -6 to 6
- output_gate_logits: bfloat16 [8192, 2048], P('sp', 'tp'), may hold values from -6 to 6
- log_input_gate: float32 [16, 8192], P('tp', 'sp'), may hold values from -4 to 104, as said below
- forget_gate_logits: float32 [16, 8192], P('tp', 'sp'), may hold values from 1 to 20
- extra_forget_terms: float32 [16, 8192], P('tp', 'sp'), may hold values from -2.1 to 0, as said below
- per_head_norm_gain: float32 [2048], P('tp'), may hold values from 0.1 to 1.9
- output_weight: bfloat16 [2048, 2048], P('tp'), may hold values from -0.125 to 0.125
- residual: bfloat16 [8192, 2048], P(('sp', 'tp')), may hold values from -6 to 6
- after_cell_norm_gain: float32 [2048], replicated, may hold values from 0.1 to 1.9
- feedforward_norm_gain: float32 [2048], replicated, may hold values from 0.1 to 1.9
- closing_norm_gain: float32 [2048], replicated, may hold values from 0.1 to 1.9
- gate_up_weight: bfloat16 [2048, 5632], P('sp', 'tp'), may hold values from -0.125 to 0.125
- value_up_weight: bfloat16 [2048, 5632], P('sp', 'tp'), may hold values from -0.125 to 0.125
- gate_filter_taps: bfloat16 [3, 5632], P(None, 'tp'), may hold values from -3 to 3
- value_filter_taps: bfloat16 [3, 5632], P(None, 'tp'), may hold values from -3 to 3
- down_weight: bfloat16 [5632, 2048], P('tp', 'sp'), may hold values from -0.078125 to 0.078125
Outputs:
- result: bfloat16 [8192, 2048], P(('sp', 'tp'))
The draws below stay inside these ranges and needn't reach their ends.
Inputs may be any that keep to these rules, and one draw needn't show every extreme that they name: log_input_gate is a log gate of order one at most positions and may be far larger at a few. extra_forget_terms is zero at nearly all positions.
All inputs are finite; a program needn't handle non-finite values.
Results may differ from the reference program's by a relative error of at most 0.019.
Values may be sent and summed in bfloat16 or wider, within the bound.
A program may use at most 128 MiB of HBM per device.

```python
import jax
import jax.numpy as jnp
from jax import lax

D = 2048
HEADS = 16
KEY_DIM = 64
VAL_DIM = 128
FF = 5632
WIDTH = 3
BLOCK = 64
TOK_DEV = 1024
TOKENS = 8192
N_TP = 4


def draw_log_input_gate(key, part):
    first = jax.random.fold_in(key, 0)
    return jax.random.truncated_normal(first, -4.0, 4.0, (HEADS, TOKENS), jnp.float32)


def draw_forget_gate_logits(key, part):
    parts_keys = jax.random.split(key, 5)
    share = 0.5
    slow = jax.random.uniform(parts_keys[0], (HEADS, 1), jnp.float32) < share
    slow_rate = jax.random.uniform(parts_keys[1], (HEADS, 1), jnp.float32, 0.2, 0.8) / TOKENS
    fast_rate = jax.random.uniform(parts_keys[2], (HEADS, 1), jnp.float32, 0.01, 0.033)
    blocks = TOKENS // TOK_DEV
    factor = jnp.exp(jax.random.uniform(parts_keys[3], (1, blocks), jnp.float32, -0.7, 0.7))
    factor = jnp.repeat(factor, TOK_DEV, axis=1)
    noise = jnp.exp(0.5 * jax.random.truncated_normal(parts_keys[4], -2.0, 2.0, (HEADS, TOKENS), jnp.float32))
    rate = jnp.where(slow, slow_rate, fast_rate) * factor * noise
    return -jnp.log(jnp.expm1(rate))


def draw_extra_forget_terms(key, part):
    first, second = jax.random.split(key, 2)
    spots = jax.random.randint(first, (HEADS, 3), 0, TOKENS)
    drops = -jax.random.uniform(second, (HEADS, 3), jnp.float32, 0.22, 0.69)
    places = jnp.arange(TOKENS)[None, None, :] == spots[:, :, None]
    return jnp.sum(jnp.where(places, drops[:, :, None], 0.0), axis=1)


def shard_levels(key, extent, pieces, smallest, top_value):
    factor_of = 1.0
    for position, parts in pieces:
        steps = jax.random.uniform(jax.random.fold_in(jax.random.fold_in(key, 6), position), (parts,), jnp.float32, smallest / len(pieces), top_value / len(pieces))
        factor_of = factor_of * jnp.repeat(jnp.exp(steps), extent[position] // parts).reshape((-1,) + (1,) * (len(extent) - 1 - position))
    return factor_of


def gaussian(own_key, dims, width, reach, shards=(), kind=jnp.bfloat16):
    factor_of = shard_levels(own_key, dims, shards, -0.22, 0.18) if shards else 1.0
    drawn = jax.random.normal(own_key, dims, jnp.float32) * width * factor_of
    return jnp.minimum(jnp.maximum(drawn, -reach), reach).astype(kind)


def setup_inputs(seed: int = 0) -> dict:
    seeds = jax.random.split(jax.random.key(seed), 19)
    return {
        "queries": gaussian(seeds[0], (TOKENS, HEADS * KEY_DIM), 1.0, 6.0, ((0, 8), (1, 4))),
        "keys": gaussian(seeds[1], (TOKENS, HEADS * KEY_DIM), 1.0, 6.0, ((0, 8), (1, 4))),
        "values": gaussian(seeds[2], (TOKENS, HEADS * VAL_DIM), 1.0, 6.0, ((0, 8), (1, 4))),
        "output_gate_logits": gaussian(seeds[3], (TOKENS, HEADS * VAL_DIM), 1.0, 6.0, ((0, 8), (1, 4))),
        "log_input_gate": draw_log_input_gate(jax.random.fold_in(seeds[18], 71), 0),
        "forget_gate_logits": draw_forget_gate_logits(jax.random.fold_in(seeds[18], 71), 0),
        "extra_forget_terms": draw_extra_forget_terms(jax.random.fold_in(seeds[18], 71), 0),
        "per_head_norm_gain": jnp.clip(1.0 + 0.18 * jax.random.normal(seeds[7], (HEADS * VAL_DIM,), jnp.float32), 0.1, 1.9),
        "output_weight": gaussian(seeds[8], (HEADS * VAL_DIM, D), (HEADS * VAL_DIM) ** -0.5, 0.125, ((0, 4),)),
        "residual": gaussian(seeds[9], (TOKENS, D), 1.0, 6.0, ((0, 32),)),
        "after_cell_norm_gain": jnp.clip(1.0 + 0.18 * jax.random.normal(seeds[10], (D,), jnp.float32), 0.1, 1.9),
        "feedforward_norm_gain": jnp.clip(1.0 + 0.18 * jax.random.normal(seeds[11], (D,), jnp.float32), 0.1, 1.9),
        "closing_norm_gain": jnp.clip(1.0 + 0.18 * jax.random.normal(seeds[12], (D,), jnp.float32), 0.1, 1.9),
        "gate_up_weight": gaussian(seeds[13], (D, FF), D ** -0.5, 0.125, ((0, 8), (1, 4))),
        "value_up_weight": gaussian(seeds[14], (D, FF), D ** -0.5, 0.125, ((0, 8), (1, 4))),
        "gate_filter_taps": gaussian(seeds[15], (WIDTH, FF), 0.577, 3.0, ((1, 4),)),
        "value_filter_taps": gaussian(seeds[16], (WIDTH, FF), 0.577, 3.0, ((1, 4),)),
        "down_weight": gaussian(seeds[17], (FF, D), FF ** -0.5, 0.078125, ((0, 4), (1, 8))),
    }


eps = 1e-06
exact_mode = lax.Precision.HIGHEST

def block_step(carried_in, inputs):
    state_cells, state_norm, state_max = carried_in
    queries_blk, keys_blk, values_blk, gate_in, gate_log = inputs
    span_len = queries_blk.shape[1]
    causal = jnp.tril(jnp.ones((span_len, span_len), dtype=bool))
    cum_log = jnp.cumsum(gate_log, axis=-1)
    decay_log = jnp.where(causal, cum_log[:, :, None] - cum_log[:, None, :] + gate_in[:, None, :], -jnp.inf)
    carried_log = cum_log + state_max[:, None]
    top_log = jnp.maximum(carried_log, lax.optimization_barrier(jnp.max(decay_log, axis=-1)))
    scores = jnp.einsum('htd,hsd->hts', queries_blk, keys_blk, precision=exact_mode) * jnp.exp(decay_log - top_log[:, :, None])
    carried_weight = jnp.exp(carried_log - top_log)
    numerator = jnp.einsum('hts,hse->hte', scores, values_blk, precision=exact_mode)
    numerator = numerator + carried_weight[:, :, None] * jnp.einsum('htd,hde->hte', queries_blk, state_cells, precision=exact_mode)
    denominator = lax.optimization_barrier(jnp.sum(scores, axis=-1)) + carried_weight * jnp.einsum('htd,hd->ht', queries_blk, state_norm, precision=exact_mode)
    output = numerator / jnp.maximum(jnp.abs(denominator), jnp.exp(-top_log))[:, :, None]
    last_log = cum_log[:, -1]
    gain_log = last_log[:, None] - cum_log + gate_in
    next_max = jnp.maximum(last_log + state_max, lax.optimization_barrier(jnp.max(gain_log, axis=-1)))
    fade_out = jnp.exp(last_log + state_max - next_max)
    weighted = jnp.exp(gain_log - next_max[:, None])[:, :, None] * keys_blk
    next_cells = fade_out[:, None, None] * state_cells + jnp.einsum('hsd,hse->hde', weighted, values_blk, precision=exact_mode)
    next_norm = fade_out[:, None] * state_norm + lax.optimization_barrier(jnp.sum(weighted, axis=1))
    return ((next_cells, next_norm, next_max), output)

def split_heads(array, head_count, head_width, blocks):
    return array.astype(jnp.float32).reshape(blocks, BLOCK, head_count, head_width).transpose(0, 2, 1, 3)

def gate_blocks(array, blocks):
    return array.reshape(array.shape[0], blocks, BLOCK).transpose(1, 0, 2)

def rms_gain(inputs, gains):
    return inputs * lax.rsqrt(lax.optimization_barrier(jnp.mean(inputs * inputs, axis=-1, keepdims=True)) + eps) * gains

def split_sum(left_side, right_side, shard_count):
    shard_width = left_side.shape[1] // shard_count
    running = jnp.zeros((left_side.shape[0], right_side.shape[1]), jnp.float32)
    for shard_idx in range(shard_count):
        lower = shard_idx * shard_width
        part_sum = jnp.dot(left_side[:, lower:lower + shard_width], right_side[lower:lower + shard_width], preferred_element_type=jnp.float32)
        rounded = lax.optimization_barrier(part_sum.astype(jnp.bfloat16))
        running = running + rounded.astype(jnp.float32)
    return running

def causal_conv(rows_in, kernel_taps):
    length = rows_in.shape[0]
    padded = jnp.pad(rows_in.astype(jnp.float32), ((WIDTH - 1, 0), (0, 0)))
    summed = jnp.zeros(rows_in.shape, jnp.float32)
    for offset in range(WIDTH):
        summed = summed + kernel_taps[offset].astype(jnp.float32) * padded[offset:offset + length]
    return summed

def reference(queries, keys, values, output_gate_logits, log_input_gate, forget_gate_logits, extra_forget_terms, per_head_norm_gain, output_weight, residual, after_cell_norm_gain, feedforward_norm_gain, closing_norm_gain, gate_up_weight, value_up_weight, gate_filter_taps, value_filter_taps, down_weight):
    blocks = TOKENS // BLOCK
    query_scale = KEY_DIM ** (-0.5)
    queries_f = split_heads(queries, HEADS, KEY_DIM, blocks) * query_scale
    keys_f = split_heads(keys, HEADS, KEY_DIM, blocks)
    values_f = split_heads(values, HEADS, VAL_DIM, blocks)
    log_forget_terms = jax.nn.log_sigmoid(forget_gate_logits) + extra_forget_terms
    start = (jnp.zeros((HEADS, KEY_DIM, VAL_DIM), jnp.float32), jnp.zeros((HEADS, KEY_DIM), jnp.float32), jnp.zeros((HEADS,), jnp.float32))
    _, cell_out = lax.scan(block_step, start, (queries_f, keys_f, values_f, gate_blocks(log_input_gate, blocks), gate_blocks(log_forget_terms, blocks)))
    cell_out = cell_out.transpose(0, 2, 1, 3).reshape(TOKENS, HEADS * VAL_DIM)
    mixed = cell_out * per_head_norm_gain * jax.nn.sigmoid(output_gate_logits.astype(jnp.float32))
    mixed = mixed.astype(jnp.bfloat16)
    mixer_out = split_sum(mixed, output_weight, N_TP).astype(jnp.bfloat16)
    after_mixer = (residual.astype(jnp.float32) + rms_gain(mixer_out.astype(jnp.float32), after_cell_norm_gain)).astype(jnp.bfloat16)
    normed = rms_gain(after_mixer.astype(jnp.float32), feedforward_norm_gain).astype(jnp.bfloat16)
    gate_rows = jnp.dot(normed, gate_up_weight, preferred_element_type=jnp.float32).astype(jnp.bfloat16)
    value_rows = jnp.dot(normed, value_up_weight, preferred_element_type=jnp.float32).astype(jnp.bfloat16)
    gate_conv = causal_conv(gate_rows, gate_filter_taps)
    value_conv = causal_conv(value_rows, value_filter_taps)
    activated = (jax.nn.gelu(gate_conv, approximate=True) * value_conv).astype(jnp.bfloat16)
    ffn_out = split_sum(activated, down_weight, N_TP).astype(jnp.bfloat16)
    return (after_mixer.astype(jnp.float32) + rms_gain(ffn_out.astype(jnp.float32), closing_norm_gain)).astype(jnp.bfloat16)
```

```python
import functools

import jax
import jax.numpy as jnp
from jax import lax
from jax.experimental import pallas as pl
from jax.experimental.pallas import tpu as pltpu
from jax.sharding import PartitionSpec as P

MESH = pl.DeviceIdType.MESH
CORES = 2
KEY_DIM = 64
VAL_DIM = 128
WIDTH = 3
LANES = 128
CHUNK = 128
HALO = 16
VMEM_BYTES = 67_000_000

eps = 1e-06
empty_log = -1e30
f32, bf16 = jnp.float32, jnp.bfloat16


def rms_scale(total_square, width):
    return lax.rsqrt(total_square / width + eps)


def rms_gain(inputs, gains):
    return inputs * lax.rsqrt(jnp.mean(inputs * inputs, axis=-1, keepdims=True) + eps) * gains


def remote(src, dst, send, recv, where):
    return pltpu.make_async_remote_copy(
        src_ref=src,
        dst_ref=dst,
        send_sem=send,
        recv_sem=recv,
        device_id=where,
        device_id_type=MESH,
    )


def mm(left, right):
    return jnp.dot(left, right, preferred_element_type=f32)


def split(array):
    high = array.astype(bf16)
    return high, (array - high.astype(f32)).astype(bf16)


def scan_lanes(array, op, neutral):
    length = array.shape[1]
    lane = lax.broadcasted_iota(jnp.int32, array.shape, 1)
    shift = 1
    while shift < length:
        moved = pltpu.roll(array, shift, 1)
        array = op(array, jnp.where(lane >= shift, moved, neutral))
        shift *= 2
    return array


def grid_of(count):
    rows_y = 1
    while 8 * rows_y * rows_y <= count:
        rows_y *= 2
    return count // rows_y, rows_y


def to_sp(place, count):
    rows_z, rows_y = grid_of(count)
    at_y, k = place // rows_z, lax.rem(place, rows_z)
    at_z = jnp.where(lax.rem(at_y, 2) == 0, k, rows_z - 1 - k)
    return at_z * rows_y + at_y


def to_place(sp, count):
    rows_z, rows_y = grid_of(count)
    at_z, at_y = sp // rows_y, lax.rem(sp, rows_y)
    return at_y * rows_z + jnp.where(lax.rem(at_y, 2) == 0, at_z, rows_z - 1 - at_z)


def reach_of(count, way, half):
    return count // 2 if way == half else count // 2 - 1


def ring_events(count):
    ways = []
    for way in range(2):
        events = []
        for kind in ("up", "down"):
            for hop in range(1, count // 2 + 1):
                for half in range(2):
                    if hop <= reach_of(count, way, half):
                        for part in range(2 if kind == "up" else 1):
                            events.append((kind, half, part, hop))
        ways.append(events)
    return ways


class Ring:
    def __init__(self, count, up_own, up_all, down_own, down_all, send, recv):
        self.count = count
        self.up_own, self.up_all = up_own, up_all
        self.down_own, self.down_all = down_own, down_all
        self.send, self.recv = send, recv
        self.place = to_place(lax.axis_index("sp"), count)
        self.events = ring_events(count)
        self.at = [{e: i for i, e in enumerate(events)} for events in self.events]
        self.waited = set()
        self.sent = []
        self.next = 0

    def piece(self, kind, half, part, shard, own):
        if kind == "up":
            tiles, rows = self.up_own.shape[0], self.up_own.shape[1]
            low = (tiles + 1) // 2
            span = pl.ds(0, low) if part == 0 else pl.ds(low, tiles - low)
            if tiles == 1:
                return None if part else self._up(pl.ds(0, 1), half, shard, rows, own)
            return self._up(span, half, shard, rows, own)
        rows = self.down_own.shape[0] // 2
        span = pl.ds(half * rows, rows)
        return self.down_own.at[span] if own else self.down_all.at[shard, span]

    def _up(self, span, half, shard, rows, own):
        if own:
            return self.up_own.at[span, pl.ds(half * (rows // 2), rows // 2)]
        start = pl.multiple_of(shard * rows + half * (rows // 2), rows // 2)
        return self.up_all.at[span, pl.ds(start, rows // 2)]

    def shard(self, way, hop):
        step = hop if way == 0 else self.count - hop
        return to_sp(lax.rem(self.place + self.count - step, self.count), self.count)

    def copy(self, way, event, target):
        kind, half, part, hop = event
        at = self.at[way][event]
        shard = self.shard(way, hop - 1)
        src = self.piece(kind, half, part, shard, hop == 1)
        dst = self.piece(kind, half, part, shard, False)
        return remote(src, dst, self.send.at[way, at], self.recv.at[way, at], target)

    def arrived(self, way, event):
        if (way, event) in self.waited:
            return
        self.waited.add((way, event))
        kind, half, part, hop = event
        at = self.at[way][event]
        came = self.piece(kind, half, part, self.shard(way, hop), False)
        where = {"sp": self.shard(way, 1)}
        remote(came, came, self.send.at[way, at], self.recv.at[way, at], where).wait_recv()

    def pump(self, times=1):
        for _ in range(times):
            if self.next >= len(self.events[0]):
                return
            for way in range(2):
                event = self.events[way][self.next]
                kind, half, part, hop = event
                if hop > 1:
                    self.arrived(way, (kind, half, part, hop - 1))
                target = {"sp": self.shard(1 - way, 1)}
                copy = self.copy(way, event, target)
                copy.start()
                self.sent.append(copy)
            self.next += 1

    def pump_to(self, number):
        self.pump(max(number - self.next, 0))

    def arrived_all(self, kind, hop=None):
        for way in range(2):
            for event in self.events[way]:
                if event[0] == kind and (hop is None or event[3] == hop):
                    self.arrived(way, event)


def tp_places(count):
    me = lax.axis_index("tp")
    at_x, core = me // CORES, lax.rem(me, CORES)
    xs = count // CORES
    partner = at_x * CORES + 1 - core
    peers = [lax.rem(at_x + k, xs) * CORES + core for k in range(xs)]
    sources = [lax.rem(at_x + xs - k, xs) * CORES + core for k in range(xs)]
    return me, at_x, core, partner, peers, sources


def columns_of(rows):
    depth = rows.shape[0]
    if depth < LANES:
        rows = jnp.concatenate([rows, jnp.zeros((LANES - depth, LANES), f32)], axis=0)
    return rows.T


def column(turned, at):
    return jnp.broadcast_to(turned[:, at : at + 1], (turned.shape[0], LANES))


def wide(array):
    return jnp.concatenate([array, array], axis=1)


def gate_rows_into(heads, gate_ref, forget_ref, extra_ref, reach_ref, top_ref, cum_ref):
    def full(ref):
        array = ref[...]
        return jnp.concatenate([array] * (8 // heads), axis=0)

    logits = full(forget_ref)
    cum = scan_lanes(full(extra_ref) - jnp.log1p(jnp.exp(-logits)), jnp.add, 0.0)
    reach = full(gate_ref) - cum
    cum_ref[...] = cum
    reach_ref[...] = reach
    top_ref[...] = scan_lanes(reach, jnp.maximum, empty_log)


def cell_block(heads, b, q_ref, k_ref, v_ref, reach_ref, top_ref, num_ref, den_ref, state_ref, held_ref):
    rows = pl.ds(pl.multiple_of(b * CHUNK, CHUNK), CHUNK)
    reach, top = reach_ref[:, rows], top_ref[:, rows]
    before = held_ref[...]
    now = jnp.broadcast_to(jnp.max(top, axis=1, keepdims=True), top.shape)
    held_ref[...] = now
    turned = columns_of(jnp.concatenate([top, jnp.exp(before - top)], axis=0))
    fade = jnp.exp(before - now)
    weight = jnp.exp(reach - now)
    at_t = lax.broadcasted_iota(jnp.int32, (CHUNK, CHUNK), 0)
    at_s = lax.broadcasted_iota(jnp.int32, (CHUNK, CHUNK), 1)
    causal = at_s <= at_t
    ones = jnp.ones((CHUNK, LANES), bf16)
    for pair in range(heads // 2):
        pair_cols = pl.ds(pair * LANES, LANES)
        query = q_ref[rows, pair_cols]
        turned_keys = k_ref[rows, pair_cols].astype(f32).T
        for h in (2 * pair, 2 * pair + 1):
            cols = pl.ds(h * VAL_DIM, VAL_DIM)
            value = jnp.concatenate([v_ref[rows, cols], ones], axis=1)
            own = (at_t >= KEY_DIM) if h % 2 else (at_t < KEY_DIM)
            keys = jnp.where(own, turned_keys, 0.0)
            decay = jnp.exp(jnp.where(causal, reach[h : h + 1, :] - column(turned, h), empty_log))
            high, low = split(mm(query, keys.astype(bf16)) * decay)
            state = state_ref[h]
            state_high, state_low = split(state)
            carried = mm(query, state_high) + mm(query, state_low)
            total = mm(high, value) + mm(low, value) + wide(column(turned, 8 + h)) * carried
            num_ref[rows, cols] = total[:, :LANES]
            den_ref[rows, cols] = total[:, LANES:]
            high, low = split(keys * weight[h : h + 1, :])
            state_ref[h] = state * wide(fade[h : h + 1, :]) + mm(high, value) + mm(low, value)


def pack_state(heads, state_ref, held_ref, cum_last, cells_ref, small_ref):
    pairs = heads // 2
    rows = []
    for pair in range(pairs):
        both = state_ref[2 * pair] + state_ref[2 * pair + 1]
        cells_ref[pair] = both[:, :LANES]
        rows.append(both[:, LANES:].T[0:1, :])
    tops = held_ref[0:heads, :] + cum_last[0:heads, :]
    rows += [tops, cum_last[0:heads, :]]
    used = pairs + 2 * heads
    rows.append(jnp.zeros((small_ref.shape[0] - used, LANES), f32))
    small_ref[...] = jnp.concatenate(rows, axis=0)


def merge_state(heads, cells_ref, small_ref, in_cells, in_norm, in_top, in_after):
    pairs = heads // 2
    small = small_ref[...]
    tops, totals = small[pairs : pairs + heads, :], small[pairs + heads : pairs + 2 * heads, :]
    top, after = in_top[0:heads, :], in_after[0:heads, :]
    reach = after + tops
    best = jnp.maximum(top, reach)
    old, new = jnp.exp(top - best), jnp.exp(reach - best)
    in_top[0:heads, :] = best
    in_after[0:heads, :] = after + totals
    lane = lax.broadcasted_iota(jnp.int32, (1, LANES), 1) < KEY_DIM
    row = lax.broadcasted_iota(jnp.int32, (LANES, LANES), 0) < KEY_DIM
    for pair in range(pairs):
        a, b = slice(2 * pair, 2 * pair + 1), slice(2 * pair + 1, 2 * pair + 2)
        in_norm[pair : pair + 1, :] = (
            jnp.where(lane, old[a], old[b]) * in_norm[pair : pair + 1, :]
            + jnp.where(lane, new[a], new[b]) * small[pair : pair + 1, :]
        )
        in_cells[pair] = (
            jnp.where(row, old[a], old[b]) * in_cells[pair]
            + jnp.where(row, new[a], new[b]) * cells_ref[pair]
        )


def mix_block(
    heads, b, q_ref, gate_ref, gain_ref, top_ref, cum_ref, num_ref, den_ref, in_top, enter_ref, mixed_ref
):
    rows = pl.ds(pl.multiple_of(b * CHUNK, CHUNK), CHUNK)
    top, cum, came = top_ref[:, rows], cum_ref[:, rows], in_top[...]
    best = jnp.maximum(top, came)
    turned = columns_of(
        jnp.concatenate([jnp.exp(top - best), jnp.exp(came - best), jnp.exp(-(cum + best))], axis=0)
    )
    scale = KEY_DIM ** (-0.5)
    for pair in range(heads // 2):
        query = q_ref[rows, pl.ds(pair * LANES, LANES)]
        for h in (2 * pair, 2 * pair + 1):
            cols = pl.ds(h * VAL_DIM, VAL_DIM)
            carried = mm(query, enter_ref[0, h]) + mm(query, enter_ref[1, h])
            here, there, floor = column(turned, h), column(turned, 8 + h), column(turned, 16 + h)
            num = (here * num_ref[rows, cols] + there * carried[:, :LANES]) * scale
            den = (here * den_ref[rows, cols] + there * carried[:, LANES:]) * scale
            out = num / jnp.maximum(jnp.abs(den), floor)
            gate = jax.nn.sigmoid(gate_ref[rows, cols].astype(f32))
            mixed_ref[rows, cols] = (out * gain_ref[:, cols] * gate).astype(bf16)


def step_kernel(
    count, sps, pieces,
    q_ref, k_ref, v_ref, out_gate_ref, in_gate_ref, forget_ref, extra_ref, head_gain_ref,
    out_weight_ref, residual_ref, cell_gain_ref, ffn_gain_ref, close_gain_ref,
    up_own, gate_taps_ref, value_taps_ref, down_own,
    out_ref,
    up_all, down_all,
    reach_ref, top_ref, cum_ref, num_ref, den_ref, state_ref, held_ref,
    cells_out, small_out, cells_in, small_in, in_cells, in_norm, in_top, in_after, enter_ref,
    mixed_ref, total, pair_out, pair_in, x_out, x_in, after_ref, normed_ref, lift_ref, active_ref,
    total2, pair_out2, pair_in2, x_out2, x_in2,
    ring_send, ring_recv, own_sems, s_send, s_recv, t_send, t_recv, h_sems,
    pair_send, pair_recv, x_send, x_recv, gx_send, gx_recv, gp_send, gp_recv,
    p2_send, p2_recv, x2_send, x2_recv,
):
    sp = lax.axis_index("sp")
    me, at_x, core, partner, peers, sources = tp_places(count)
    xs = count // CORES
    tok_rows, heads = q_ref.shape[0], in_gate_ref.shape[0]
    blocks = tok_rows // CHUNK
    rows = tok_rows // count
    step = rows // pieces
    width = out_weight_ref.shape[1]
    ring = Ring(sps, up_own, up_all, down_own, down_all, ring_send, ring_recv)

    barrier = pltpu.get_barrier_semaphore()
    for d in range(1, sps):
        pl.semaphore_signal(
            barrier, inc=1, device_id={"sp": lax.rem(sp + d, sps)}, device_id_type=MESH
        )
    for where in [partner] + peers[1:]:
        pl.semaphore_signal(barrier, inc=1, device_id={"tp": where}, device_id_type=MESH)
    pl.semaphore_wait(barrier, sps - 1 + xs)

    ring.pump_to(PUMP_START)
    own_rows = up_own.shape[1]
    own_up = pltpu.make_async_copy(
        up_own,
        up_all.at[:, pl.ds(pl.multiple_of(sp * own_rows, own_rows), own_rows)],
        own_sems.at[0],
    )
    own_up.start()
    own_down = pltpu.make_async_copy(down_own, down_all.at[sp], own_sems.at[1])
    own_down.start()

    gate_rows_into(heads, in_gate_ref, forget_ref, extra_ref, reach_ref, top_ref, cum_ref)
    state_ref[...] = jnp.zeros_like(state_ref)
    held_ref[...] = jnp.full_like(held_ref, empty_log)

    @pl.loop(0, blocks)
    def _(b):
        cell_block(
            heads, b, q_ref, k_ref, v_ref, reach_ref, top_ref, num_ref, den_ref, state_ref, held_ref
        )

    last = cum_ref[:, pl.ds(tok_rows - LANES, LANES)]
    cum_last = jnp.broadcast_to(last[:, LANES - 1 :], last.shape)
    pack_state(heads, state_ref, held_ref, cum_last, cells_out, small_out)
    for d in range(1, sps):
        ahead = {"sp": lax.rem(sp + d, sps)}

        @pl.when(sp + d < sps)
        def _(d=d, ahead=ahead):
            remote(small_out, small_in.at[d], t_send.at[d], t_recv.at[d], ahead).start()
            remote(cells_out, cells_in.at[d], s_send.at[d], s_recv.at[d], ahead).start()

    ring.pump_to(PUMP_STATE)
    in_cells[...] = jnp.zeros_like(in_cells)
    in_norm[...] = jnp.zeros_like(in_norm)
    in_top[...] = jnp.full_like(in_top, empty_log)
    in_after[...] = jnp.zeros_like(in_after)
    for d in range(1, sps):

        @pl.when(sp - d >= 0)
        def _(d=d):
            behind = {"sp": lax.rem(sp + sps - d, sps)}
            remote(small_out, small_in.at[d], t_send.at[d], t_recv.at[d], behind).wait_recv()
            remote(cells_out, cells_in.at[d], s_send.at[d], s_recv.at[d], behind).wait_recv()
            merge_state(
                heads, cells_in.at[d], small_in.at[d], in_cells, in_norm, in_top, in_after
            )

    for pair in range(heads // 2):
        norm = jnp.broadcast_to(in_norm[pair : pair + 1, :], (LANES, LANES)).T
        full = jnp.concatenate([in_cells[pair], norm], axis=1)
        row = lax.broadcasted_iota(jnp.int32, full.shape, 0)
        for h in (2 * pair, 2 * pair + 1):
            own = (row >= KEY_DIM) if h % 2 else (row < KEY_DIM)
            high, low = split(jnp.where(own, full, 0.0))
            enter_ref[0, h] = high
            enter_ref[1, h] = low
    ring.pump_to(PUMP_MIX)

    @pl.loop(0, blocks)
    def _(b):
        mix_block(
            heads, b, q_ref, out_gate_ref, head_gain_ref, top_ref, cum_ref, num_ref, den_ref,
            in_top, enter_ref, mixed_ref,
        )

    tile = 512 if width % 512 == 0 else width

    def product(chunk, piece, store):
        start = pl.multiple_of(chunk * rows + piece * step, step)
        left = mixed_ref[pl.ds(start, step), :]

        @pl.loop(0, width // tile)
        def _(j):
            cols = pl.ds(pl.multiple_of(j * tile, tile), tile)
            store(cols, mm(left, out_weight_ref[:, cols]))

    sent, landing = [], []
    done = 0
    for k in list(range(1, xs)) + [0]:
        to_x = lax.rem(at_x + k, xs)
        for s in range(pieces):
            span = pl.ds(s * step, step)

            def put_pair(cols, block, k=k, span=span):
                pair_out[k, span, cols] = block.astype(bf16)

            product(to_x * CORES + 1 - core, s, put_pair)
            copy = remote(
                pair_out.at[k, span], pair_in.at[k, span],
                pair_send.at[k, s], pair_recv.at[k, s], {"tp": partner},
            )
            copy.start()
            sent.append(copy)

            def put_own(cols, block, span=span):
                total[span, cols] = block.astype(bf16).astype(f32)

            product(to_x * CORES + core, s, put_own)
            copy.wait_recv()
            summed = total[span, :] + pair_in[k, span, :].astype(f32)
            if k == 0:
                total[span, :] = summed
            else:
                x_out[k - 1, span, :] = summed.astype(bf16)
                copy = remote(
                    x_out.at[k - 1, span], x_in.at[k - 1, span],
                    x_send.at[k, s], x_recv.at[k, s], {"tp": peers[k]},
                )
                copy.start()
                sent.append(copy)
                landing.append((s, copy))
    ring.pump_to(PUMP_REDUCED)

    def block(device, s):
        start = pl.multiple_of(HALO + device * rows + s * step, HALO)
        return normed_ref.at[pl.ds(start, step)]

    for s in range(pieces):
        span = pl.ds(s * step, step)
        for at, copy in landing:
            if at == s:
                copy.wait_recv()
        summed = total[span, :]
        for k in range(1, xs):
            summed = summed + x_in[k - 1, span, :].astype(f32)
        mixer_out = summed.astype(bf16).astype(f32)
        after = residual_ref[span, :].astype(f32) + rms_gain(mixer_out, cell_gain_ref[...])
        after = after.astype(bf16)
        after_ref[span, :] = after
        normed = rms_gain(after.astype(f32), ffn_gain_ref[...])
        start = pl.multiple_of(HALO + me * rows + s * step, HALO)
        normed_ref[pl.ds(start, step), :] = normed.astype(bf16)
        own = block(me, s)
        for k in range(1, xs):
            sent.append(remote(own, own, gx_send.at[k, s], gx_recv.at[k, s], {"tp": peers[k]}))
            sent[-1].start()
        sent.append(remote(own, own, gp_send.at[0, s], gp_recv.at[0, s], {"tp": partner}))
        sent[-1].start()
        ring.pump_to(PUMP_NORM[s])
    for s in range(pieces):
        for k in range(1, xs):
            came = block(sources[k], s)
            remote(came, came, gx_send.at[k, s], gx_recv.at[k, s], {"tp": peers[k]}).wait_recv()
            sent.append(remote(came, came, gp_send.at[k, s], gp_recv.at[k, s], {"tp": partner}))
            sent[-1].start()
        ring.pump_to(PUMP_GATHER[s])
    for s in range(pieces):
        for k in range(xs):
            came = block(sources[k] + partner - me, s)
            remote(came, came, gp_send.at[k, s], gp_recv.at[k, s], {"tp": partner}).wait_recv()

    ahead, behind = lax.rem(sp + 1, sps), lax.rem(sp + sps - 1, sps)
    tail = normed_ref.at[pl.ds(tok_rows, HALO)]
    head = normed_ref.at[pl.ds(0, HALO)]

    @pl.when(sp + 1 < sps)
    def _():
        remote(tail, head, h_sems.at[0], h_sems.at[1], {"sp": ahead}).start()

    @pl.when(sp == 0)
    def _():
        normed_ref[pl.ds(0, HALO), :] = jnp.zeros((HALO, width), bf16)

    ring.pump_to(PUMP_UP)
    own_up.wait()
    ring.arrived_all("up")

    @pl.when(sp > 0)
    def _():
        remote(tail, head, h_sems.at[0], h_sems.at[1], {"sp": behind}).wait_recv()

    tiles, half = up_own.shape[0], up_own.shape[2] // 2

    def up_tile(j, cols):
        lift_ref[...] = mm(normed_ref[...], up_all[j]).astype(bf16).astype(f32)
        sums = []
        for taps, side in ((gate_taps_ref, 0), (value_taps_ref, 1)):
            summed = jnp.zeros((tok_rows, half), f32)
            for offset in range(WIDTH):
                tap = taps[offset : offset + 1, cols].astype(f32)
                at = pl.ds(HALO - WIDTH + 1 + offset, tok_rows)
                summed = summed + tap * lift_ref[at, pl.ds(side * half, half)]
            sums.append(summed)
        active_ref[:, cols] = (jax.nn.gelu(sums[0], approximate=True) * sums[1]).astype(bf16)

    if half % LANES == 0:
        edges = [tiles * i // len(PUMP_TILES) for i in range(len(PUMP_TILES) + 1)]
        for i, number in enumerate(PUMP_TILES):

            @pl.loop(edges[i], edges[i + 1])
            def _(j):
                up_tile(j, pl.ds(pl.multiple_of(j * half, half), half))

            ring.pump_to(number)
    else:
        for j in range(tiles):
            up_tile(j, pl.ds(j * half, half))

    own_down.wait()

    def close_columns(shard, slot):
        copies = []
        weight = down_all[shard]
        order = list(range(1, xs)) + [0]
        for k in order:
            chunk = lax.rem(at_x + k, xs) * CORES + 1 - core
            left = active_ref[pl.ds(pl.multiple_of(chunk * rows, rows), rows), :]
            pair_out2[shard, k] = mm(left, weight).astype(bf16)
            copy = remote(
                pair_out2.at[shard, k], pair_in2.at[shard, k],
                p2_send.at[slot, k], p2_recv.at[slot, k], {"tp": partner},
            )
            copy.start()
            copies.append(copy)
        for at, k in enumerate(order):
            chunk = lax.rem(at_x + k, xs) * CORES + core
            left = active_ref[pl.ds(pl.multiple_of(chunk * rows, rows), rows), :]
            part = mm(left, weight).astype(bf16).astype(f32)
            copies[at].wait_recv()
            summed = part + pair_in2[shard, k].astype(f32)
            if k == 0:
                total2[shard] = summed
            else:
                x_out2[shard, k - 1] = summed.astype(bf16)
                copy = remote(
                    x_out2.at[shard, k - 1], x_in2.at[shard, k - 1],
                    x2_send.at[slot, k], x2_recv.at[slot, k], {"tp": peers[k]},
                )
                copy.start()
                final.append(copy)
        sent.extend(copies)

    final = []
    close_columns(sp, 0)
    slot = 1
    for hop in range(1, sps // 2 + 1):
        for way in range(2):
            if hop == sps // 2 and way == 1:
                continue
            for event in ring.events[way]:
                if event[0] == "down" and event[3] == hop:
                    ring.arrived(way, event)
            if hop == sps // 2:
                for event in ring.events[1]:
                    if event[0] == "down" and event[3] == hop:
                        ring.arrived(1, event)
            if way == 0 or hop == sps // 2:
                ring.pump(1)
            close_columns(ring.shard(way, hop), slot)
            slot += 1
            ring.pump(1)
    ring.pump(len(ring.events[0]))
    for copy in final:
        copy.wait_recv()
    square = jnp.zeros((rows, 1), f32)
    for n in range(sps):
        summed = total2[n]
        for k in range(1, xs):
            summed = summed + x_in2[n, k - 1].astype(f32)
        summed = summed.astype(bf16).astype(f32)
        total2[n] = summed
        square = square + jnp.sum(summed * summed, axis=-1, keepdims=True)
    scale = rms_scale(square, width)
    part = width // sps
    for n in range(sps):
        cols = slice(n * part, (n + 1) * part)
        result = after_ref[:, cols].astype(f32) + total2[n] * scale * close_gain_ref[:, cols]
        out_ref[:, cols] = result.astype(bf16)
    for copy in sent + final + ring.sent:
        copy.wait_send()
    for d in range(1, sps):

        @pl.when(sp + d < sps)
        def _(d=d):
            ahead = {"sp": lax.rem(sp + d, sps)}
            remote(small_out, small_in.at[d], t_send.at[d], t_recv.at[d], ahead).wait_send()
            remote(cells_out, cells_in.at[d], s_send.at[d], s_recv.at[d], ahead).wait_send()

    @pl.when(sp + 1 < sps)
    def _():
        remote(tail, head, h_sems.at[0], h_sems.at[1], {"sp": ahead}).wait_send()


PUMP_START = 4
PUMP_STATE = 5
PUMP_MIX = 7
PUMP_REDUCED = 9
PUMP_NORM = (10, 10)
PUMP_GATHER = (11, 12)
PUMP_UP = 16
PUMP_TILES = (16, 17, 18, 19)


def shards(
    queries,
    keys,
    values,
    output_gate_logits,
    log_input_gate,
    forget_gate_logits,
    extra_forget_terms,
    per_head_norm_gain,
    output_weight,
    residual,
    after_cell_norm_gain,
    feedforward_norm_gain,
    closing_norm_gain,
    gate_up_weight,
    value_up_weight,
    gate_filter_taps,
    value_filter_taps,
    down_weight,
):
    count, sps = lax.axis_size("tp"), lax.axis_size("sp")
    xs = count // CORES
    tok_rows = queries.shape[0]
    heads = log_input_gate.shape[0]
    own_depth, hidden = gate_up_weight.shape
    width = output_weight.shape[1]
    own_width = down_weight.shape[1]
    rows = tok_rows // count
    pieces = 2
    half = LANES if hidden % LANES == 0 else LANES // 2
    tiles = hidden // half
    up_own = jnp.concatenate(
        [
            gate_up_weight.reshape(own_depth, tiles, half),
            value_up_weight.reshape(own_depth, tiles, half),
        ],
        axis=2,
    ).transpose(1, 0, 2)
    events = len(ring_events(sps)[0])
    vmem = pl.BlockSpec(memory_space=pltpu.VMEM)
    hbm = pl.BlockSpec(memory_space=pl.ANY)
    dma = pltpu.SemaphoreType.DMA
    V = pltpu.VMEM
    small = -(-(heads // 2 + 2 * heads) // 8) * 8
    pairs = heads // 2
    return pl.pallas_call(
        functools.partial(step_kernel, count, sps, pieces),
        out_shape=jax.ShapeDtypeStruct(residual.shape, bf16),
        in_specs=[vmem] * 13 + [hbm, vmem, vmem, hbm],
        out_specs=vmem,
        scratch_shapes=[
            V((tiles, own_depth * sps, 2 * half), bf16),
            V((sps, hidden, own_width), bf16),
            V((8, tok_rows), f32),
            V((8, tok_rows), f32),
            V((8, tok_rows), f32),
            V((tok_rows, heads * VAL_DIM), f32),
            V((tok_rows, heads * VAL_DIM), f32),
            V((heads, LANES, 2 * LANES), f32),
            V((8, LANES), f32),
            V((pairs, LANES, LANES), f32),
            V((small, LANES), f32),
            V((sps, pairs, LANES, LANES), f32),
            V((sps, small, LANES), f32),
            V((pairs, LANES, LANES), f32),
            V((8, LANES), f32),
            V((8, LANES), f32),
            V((8, LANES), f32),
            V((2, heads, LANES, 2 * LANES), bf16),
            V((tok_rows, heads * VAL_DIM), bf16),
            V((rows, width), f32),
            V((xs, rows, width), bf16),
            V((xs, rows, width), bf16),
            V((max(xs - 1, 1), rows, width), bf16),
            V((max(xs - 1, 1), rows, width), bf16),
            V((rows, width), bf16),
            V((HALO + tok_rows, width), bf16),
            V((HALO + tok_rows, 2 * half), f32),
            V((tok_rows, hidden), bf16),
            V((sps, rows, own_width), f32),
            V((sps, xs, rows, own_width), bf16),
            V((sps, xs, rows, own_width), bf16),
            V((sps, max(xs - 1, 1), rows, own_width), bf16),
            V((sps, max(xs - 1, 1), rows, own_width), bf16),
            dma((2, events)),
            dma((2, events)),
            dma((2,)),
            dma((sps,)),
            dma((sps,)),
            dma((sps,)),
            dma((sps,)),
            dma((2,)),
        ]
        + [dma((xs, pieces))] * 8
        + [dma((sps, xs))] * 4,
        compiler_params=pltpu.CompilerParams(
            collective_id=0, has_side_effects=True, vmem_limit_bytes=VMEM_BYTES
        ),
        cost_estimate=pl.CostEstimate(
            flops=6 * tok_rows * hidden * width, bytes_accessed=3 * 10**7, transcendentals=0
        ),
        name="step",
    )(
        queries, keys, values, output_gate_logits, log_input_gate, forget_gate_logits,
        extra_forget_terms, per_head_norm_gain.reshape(1, -1), output_weight, residual,
        after_cell_norm_gain.reshape(1, -1), feedforward_norm_gain.reshape(1, -1),
        closing_norm_gain.reshape(1, -1), up_own, gate_filter_taps, value_filter_taps, down_weight,
    )


def solution(mesh):
    placed = (
        P("sp", "tp"),
        P("sp", "tp"),
        P("sp", "tp"),
        P("sp", "tp"),
        P("tp", "sp"),
        P("tp", "sp"),
        P("tp", "sp"),
        P("tp"),
        P("tp", None),
        P(("sp", "tp"), None),
        P(),
        P(),
        P(),
        P("sp", "tp"),
        P("sp", "tp"),
        P(None, "tp"),
        P(None, "tp"),
        P("tp", "sp"),
    )
    return jax.shard_map(
        shards, mesh=mesh, in_specs=placed, out_specs=P(("sp", "tp"), None), check_vma=False
    )
```

```python
import functools

import jax
import jax.numpy as jnp
from jax import lax
from jax.experimental import pallas as pl
from jax.experimental.pallas import tpu as pltpu
from jax.sharding import PartitionSpec as P

MESH = pl.DeviceIdType.MESH
CORES = 2
KEY_DIM = 64
VAL_DIM = 128
WIDTH = 3
LANES = 128
CHUNK = 128
HALO = 16
VMEM_BYTES = 67_000_000

eps = 1e-06
empty_log = -1e30
f32, bf16 = jnp.float32, jnp.bfloat16


def rms_scale(total_square, width):
    return lax.rsqrt(total_square / width + eps)


def rms_gain(inputs, gains):
    return inputs * lax.rsqrt(jnp.mean(inputs * inputs, axis=-1, keepdims=True) + eps) * gains


def remote(src, dst, send, recv, where):
    return pltpu.make_async_remote_copy(
        src_ref=src,
        dst_ref=dst,
        send_sem=send,
        recv_sem=recv,
        device_id=where,
        device_id_type=MESH,
    )


def mm(left, right):
    return jnp.dot(left, right, preferred_element_type=f32)


def split(array):
    high = array.astype(bf16)
    return high, (array - high.astype(f32)).astype(bf16)


def scan_lanes(array, op, neutral):
    length = array.shape[1]
    lane = lax.broadcasted_iota(jnp.int32, array.shape, 1)
    shift = 1
    while shift < length:
        moved = pltpu.roll(array, shift, 1)
        array = op(array, jnp.where(lane >= shift, moved, neutral))
        shift *= 2
    return array


def grid_of(count):
    rows_y = 1
    while 8 * rows_y * rows_y <= count:
        rows_y *= 2
    return count // rows_y, rows_y


def to_sp(place, count):
    rows_z, rows_y = grid_of(count)
    at_y, k = place // rows_z, lax.rem(place, rows_z)
    at_z = jnp.where(lax.rem(at_y, 2) == 0, k, rows_z - 1 - k)
    return at_z * rows_y + at_y


def to_place(sp, count):
    rows_z, rows_y = grid_of(count)
    at_z, at_y = sp // rows_y, lax.rem(sp, rows_y)
    return at_y * rows_z + jnp.where(lax.rem(at_y, 2) == 0, at_z, rows_z - 1 - at_z)


def reach_of(count, way, half):
    return count // 2 if way == half else count // 2 - 1


def ring_events(count):
    ways = []
    for way in range(2):
        events = []
        for kind in ("up", "down"):
            for hop in range(1, count // 2 + 1):
                for half in range(2):
                    if hop <= reach_of(count, way, half):
                        for part in range(2 if kind == "up" else 1):
                            events.append((kind, half, part, hop))
        ways.append(events)
    return ways


class Ring:
    def __init__(self, count, up_own, up_all, down_own, down_all, send, recv):
        self.count = count
        self.up_own, self.up_all = up_own, up_all
        self.down_own, self.down_all = down_own, down_all
        self.send, self.recv = send, recv
        self.place = to_place(lax.axis_index("sp"), count)
        self.events = ring_events(count)
        self.at = [{e: i for i, e in enumerate(events)} for events in self.events]
        self.waited = set()
        self.sent = []
        self.next = 0

    def piece(self, kind, half, part, shard, own):
        if kind == "up":
            tiles, rows = self.up_own.shape[0], self.up_own.shape[1]
            low = (tiles + 1) // 2
            span = pl.ds(0, low) if part == 0 else pl.ds(low, tiles - low)
            if tiles == 1:
                return None if part else self._up(pl.ds(0, 1), half, shard, rows, own)
            return self._up(span, half, shard, rows, own)
        rows = self.down_own.shape[0] // 2
        span = pl.ds(half * rows, rows)
        return self.down_own.at[span] if own else self.down_all.at[shard, span]

    def _up(self, span, half, shard, rows, own):
        if own:
            return self.up_own.at[span, pl.ds(half * (rows // 2), rows // 2)]
        start = pl.multiple_of(shard * rows + half * (rows // 2), rows // 2)
        return self.up_all.at[span, pl.ds(start, rows // 2)]

    def shard(self, way, hop):
        step = hop if way == 0 else self.count - hop
        return to_sp(lax.rem(self.place + self.count - step, self.count), self.count)

    def copy(self, way, event, target):
        kind, half, part, hop = event
        at = self.at[way][event]
        shard = self.shard(way, hop - 1)
        src = self.piece(kind, half, part, shard, hop == 1)
        dst = self.piece(kind, half, part, shard, False)
        return remote(src, dst, self.send.at[way, at], self.recv.at[way, at], target)

    def arrived(self, way, event):
        if (way, event) in self.waited:
            return
        self.waited.add((way, event))
        kind, half, part, hop = event
        at = self.at[way][event]
        came = self.piece(kind, half, part, self.shard(way, hop), False)
        where = {"sp": self.shard(way, 1)}
        remote(came, came, self.send.at[way, at], self.recv.at[way, at], where).wait_recv()

    def pump(self, times=1):
        for _ in range(times):
            if self.next >= len(self.events[0]):
                return
            for way in range(2):
                event = self.events[way][self.next]
                kind, half, part, hop = event
                if hop > 1:
                    self.arrived(way, (kind, half, part, hop - 1))
                target = {"sp": self.shard(1 - way, 1)}
                copy = self.copy(way, event, target)
                copy.start()
                self.sent.append(copy)
            self.next += 1

    def pump_to(self, number):
        self.pump(max(number - self.next, 0))

    def arrived_all(self, kind, hop=None):
        for way in range(2):
            for event in self.events[way]:
                if event[0] == kind and (hop is None or event[3] == hop):
                    self.arrived(way, event)


def tp_places(count):
    me = lax.axis_index("tp")
    at_x, core = me // CORES, lax.rem(me, CORES)
    xs = count // CORES
    partner = at_x * CORES + 1 - core
    peers = [lax.rem(at_x + k, xs) * CORES + core for k in range(xs)]
    sources = [lax.rem(at_x + xs - k, xs) * CORES + core for k in range(xs)]
    return me, at_x, core, partner, peers, sources


def columns_of(rows):
    depth = rows.shape[0]
    if depth < LANES:
        rows = jnp.concatenate([rows, jnp.zeros((LANES - depth, LANES), f32)], axis=0)
    return rows.T


def column(turned, at):
    return jnp.broadcast_to(turned[:, at : at + 1], (turned.shape[0], LANES))


def wide(array):
    return jnp.concatenate([array, array], axis=1)


def gate_rows_into(heads, gate_ref, forget_ref, extra_ref, reach_ref, top_ref, cum_ref):
    def full(ref):
        array = ref[...]
        return jnp.concatenate([array] * (8 // heads), axis=0)

    logits = full(forget_ref)
    cum = scan_lanes(full(extra_ref) - jnp.log1p(jnp.exp(-logits)), jnp.add, 0.0)
    reach = full(gate_ref) - cum
    cum_ref[...] = cum
    reach_ref[...] = reach
    top_ref[...] = scan_lanes(reach, jnp.maximum, empty_log)


def cell_block(heads, b, q_ref, k_ref, v_ref, reach_ref, top_ref, num_ref, den_ref, state_ref, held_ref):
    rows = pl.ds(pl.multiple_of(b * CHUNK, CHUNK), CHUNK)
    reach, top = reach_ref[:, rows], top_ref[:, rows]
    before = held_ref[...]
    now = jnp.broadcast_to(jnp.max(top, axis=1, keepdims=True), top.shape)
    held_ref[...] = now
    turned = columns_of(jnp.concatenate([top, jnp.exp(before - top)], axis=0))
    fade = jnp.exp(before - now)
    weight = jnp.exp(reach - now)
    at_t = lax.broadcasted_iota(jnp.int32, (CHUNK, CHUNK), 0)
    at_s = lax.broadcasted_iota(jnp.int32, (CHUNK, CHUNK), 1)
    causal = at_s <= at_t
    ones = jnp.ones((CHUNK, LANES), bf16)
    for pair in range(heads // 2):
        pair_cols = pl.ds(pair * LANES, LANES)
        query = q_ref[rows, pair_cols]
        turned_keys = k_ref[rows, pair_cols].astype(f32).T
        for h in (2 * pair, 2 * pair + 1):
            cols = pl.ds(h * VAL_DIM, VAL_DIM)
            value = jnp.concatenate([v_ref[rows, cols], ones], axis=1)
            own = (at_t >= KEY_DIM) if h % 2 else (at_t < KEY_DIM)
            keys = jnp.where(own, turned_keys, 0.0)
            decay = jnp.exp(jnp.where(causal, reach[h : h + 1, :] - column(turned, h), empty_log))
            high, low = split(mm(query, keys.astype(bf16)) * decay)
            state = state_ref[h]
            state_high, state_low = split(state)
            carried = mm(query, state_high) + mm(query, state_low)
            total = mm(high, value) + mm(low, value) + wide(column(turned, 8 + h)) * carried
            num_ref[rows, cols] = total[:, :LANES]
            den_ref[rows, cols] = total[:, LANES:]
            high, low = split(keys * weight[h : h + 1, :])
            state_ref[h] = state * wide(fade[h : h + 1, :]) + mm(high, value) + mm(low, value)


def pack_state(heads, state_ref, held_ref, cum_last, cells_ref, small_ref):
    pairs = heads // 2
    rows = []
    for pair in range(pairs):
        both = state_ref[2 * pair] + state_ref[2 * pair + 1]
        cells_ref[pair] = both[:, :LANES]
        rows.append(both[:, LANES:].T[0:1, :])
    tops = held_ref[0:heads, :] + cum_last[0:heads, :]
    rows += [tops, cum_last[0:heads, :]]
    used = pairs + 2 * heads
    rows.append(jnp.zeros((small_ref.shape[0] - used, LANES), f32))
    small_ref[...] = jnp.concatenate(rows, axis=0)


def merge_state(heads, cells_ref, small_ref, in_cells, in_norm, in_top, in_after):
    pairs = heads // 2
    small = small_ref[...]
    tops, totals = small[pairs : pairs + heads, :], small[pairs + heads : pairs + 2 * heads, :]
    top, after = in_top[0:heads, :], in_after[0:heads, :]
    reach = after + tops
    best = jnp.maximum(top, reach)
    old, new = jnp.exp(top - best), jnp.exp(reach - best)
    in_top[0:heads, :] = best
    in_after[0:heads, :] = after + totals
    lane = lax.broadcasted_iota(jnp.int32, (1, LANES), 1) < KEY_DIM
    row = lax.broadcasted_iota(jnp.int32, (LANES, LANES), 0) < KEY_DIM
    for pair in range(pairs):
        a, b = slice(2 * pair, 2 * pair + 1), slice(2 * pair + 1, 2 * pair + 2)
        in_norm[pair : pair + 1, :] = (
            jnp.where(lane, old[a], old[b]) * in_norm[pair : pair + 1, :]
            + jnp.where(lane, new[a], new[b]) * small[pair : pair + 1, :]
        )
        in_cells[pair] = (
            jnp.where(row, old[a], old[b]) * in_cells[pair]
            + jnp.where(row, new[a], new[b]) * cells_ref[pair]
        )


def mix_block(
    heads, b, q_ref, gate_ref, gain_ref, top_ref, cum_ref, num_ref, den_ref, in_top, enter_ref, mixed_ref
):
    rows = pl.ds(pl.multiple_of(b * CHUNK, CHUNK), CHUNK)
    top, cum, came = top_ref[:, rows], cum_ref[:, rows], in_top[...]
    best = jnp.maximum(top, came)
    turned = columns_of(
        jnp.concatenate([jnp.exp(top - best), jnp.exp(came - best), jnp.exp(-(cum + best))], axis=0)
    )
    scale = KEY_DIM ** (-0.5)
    for pair in range(heads // 2):
        query = q_ref[rows, pl.ds(pair * LANES, LANES)]
        for h in (2 * pair, 2 * pair + 1):
            cols = pl.ds(h * VAL_DIM, VAL_DIM)
            carried = mm(query, enter_ref[0, h]) + mm(query, enter_ref[1, h])
            here, there, floor = column(turned, h), column(turned, 8 + h), column(turned, 16 + h)
            num = (here * num_ref[rows, cols] + there * carried[:, :LANES]) * scale
            den = (here * den_ref[rows, cols] + there * carried[:, LANES:]) * scale
            out = num / jnp.maximum(jnp.abs(den), floor)
            gate = jax.nn.sigmoid(gate_ref[rows, cols].astype(f32))
            mixed_ref[rows, cols] = (out * gain_ref[:, cols] * gate).astype(bf16)


def step_kernel(
    count, sps, pieces,
    q_ref, k_ref, v_ref, out_gate_ref, in_gate_ref, forget_ref, extra_ref, head_gain_ref,
    out_weight_ref, residual_ref, cell_gain_ref, ffn_gain_ref, close_gain_ref,
    up_own, gate_taps_ref, value_taps_ref, down_own,
    out_ref,
    up_all, down_all,
    reach_ref, top_ref, cum_ref, num_ref, den_ref, state_ref, held_ref,
    cells_out, small_out, cells_in, small_in, in_cells, in_norm, in_top, in_after, enter_ref,
    mixed_ref, total, pair_out, pair_in, x_out, x_in, after_ref, normed_ref, lift_ref, active_ref,
    total2, pair_out2, pair_in2, x_out2, x_in2,
    ring_send, ring_recv, own_sems, s_send, s_recv, t_send, t_recv, h_sems,
    pair_send, pair_recv, x_send, x_recv, gx_send, gx_recv, gp_send, gp_recv,
    p2_send, p2_recv, x2_send, x2_recv,
):
    sp = lax.axis_index("sp")
    me, at_x, core, partner, peers, sources = tp_places(count)
    xs = count // CORES
    tok_rows, heads = q_ref.shape[0], in_gate_ref.shape[0]
    blocks = tok_rows // CHUNK
    rows = tok_rows // count
    step = rows // pieces
    width = out_weight_ref.shape[1]
    ring = Ring(sps, up_own, up_all, down_own, down_all, ring_send, ring_recv)

    barrier = pltpu.get_barrier_semaphore()
    for d in range(1, sps):
        pl.semaphore_signal(
            barrier, inc=1, device_id={"sp": lax.rem(sp + d, sps)}, device_id_type=MESH
        )
    for where in [partner] + peers[1:]:
        pl.semaphore_signal(barrier, inc=1, device_id={"tp": where}, device_id_type=MESH)
    pl.semaphore_wait(barrier, sps - 1 + xs)

    ring.pump_to(PUMP_START)
    own_rows = up_own.shape[1]
    own_up = pltpu.make_async_copy(
        up_own,
        up_all.at[:, pl.ds(pl.multiple_of(sp * own_rows, own_rows), own_rows)],
        own_sems.at[0],
    )
    own_up.start()
    own_down = pltpu.make_async_copy(down_own, down_all.at[sp], own_sems.at[1])
    own_down.start()

    gate_rows_into(heads, in_gate_ref, forget_ref, extra_ref, reach_ref, top_ref, cum_ref)
    state_ref[...] = jnp.zeros_like(state_ref)
    held_ref[...] = jnp.full_like(held_ref, empty_log)

    @pl.loop(0, blocks)
    def _(b):
        cell_block(
            heads, b, q_ref, k_ref, v_ref, reach_ref, top_ref, num_ref, den_ref, state_ref, held_ref
        )

    last = cum_ref[:, pl.ds(tok_rows - LANES, LANES)]
    cum_last = jnp.broadcast_to(last[:, LANES - 1 :], last.shape)
    pack_state(heads, state_ref, held_ref, cum_last, cells_out, small_out)
    for d in range(1, sps):
        ahead = {"sp": lax.rem(sp + d, sps)}

        @pl.when(sp + d < sps)
        def _(d=d, ahead=ahead):
            remote(small_out, small_in.at[d], t_send.at[d], t_recv.at[d], ahead).start()
            remote(cells_out, cells_in.at[d], s_send.at[d], s_recv.at[d], ahead).start()

    ring.pump_to(PUMP_STATE)
    in_cells[...] = jnp.zeros_like(in_cells)
    in_norm[...] = jnp.zeros_like(in_norm)
    in_top[...] = jnp.full_like(in_top, empty_log)
    in_after[...] = jnp.zeros_like(in_after)
    for d in range(1, sps):

        @pl.when(sp - d >= 0)
        def _(d=d):
            behind = {"sp": lax.rem(sp + sps - d, sps)}
            remote(small_out, small_in.at[d], t_send.at[d], t_recv.at[d], behind).wait_recv()
            remote(cells_out, cells_in.at[d], s_send.at[d], s_recv.at[d], behind).wait_recv()
            merge_state(
                heads, cells_in.at[d], small_in.at[d], in_cells, in_norm, in_top, in_after
            )

    for pair in range(heads // 2):
        norm = jnp.broadcast_to(in_norm[pair : pair + 1, :], (LANES, LANES)).T
        full = jnp.concatenate([in_cells[pair], norm], axis=1)
        row = lax.broadcasted_iota(jnp.int32, full.shape, 0)
        for h in (2 * pair, 2 * pair + 1):
            own = (row >= KEY_DIM) if h % 2 else (row < KEY_DIM)
            high, low = split(jnp.where(own, full, 0.0))
            enter_ref[0, h] = high
            enter_ref[1, h] = low
    ring.pump_to(PUMP_MIX)

    @pl.loop(0, blocks)
    def _(b):
        mix_block(
            heads, b, q_ref, out_gate_ref, head_gain_ref, top_ref, cum_ref, num_ref, den_ref,
            in_top, enter_ref, mixed_ref,
        )

    tile = 512 if width % 512 == 0 else width

    def product(chunk, piece, store):
        start = pl.multiple_of(chunk * rows + piece * step, step)
        left = mixed_ref[pl.ds(start, step), :]

        @pl.loop(0, width // tile)
        def _(j):
            cols = pl.ds(pl.multiple_of(j * tile, tile), tile)
            store(cols, mm(left, out_weight_ref[:, cols]))

    sent, landing = [], []
    done = 0
    for k in list(range(1, xs)) + [0]:
        to_x = lax.rem(at_x + k, xs)
        for s in range(pieces):
            span = pl.ds(s * step, step)

            def put_pair(cols, block, k=k, span=span):
                pair_out[k, span, cols] = block.astype(bf16)

            product(to_x * CORES + 1 - core, s, put_pair)
            copy = remote(
                pair_out.at[k, span], pair_in.at[k, span],
                pair_send.at[k, s], pair_recv.at[k, s], {"tp": partner},
            )
            copy.start()
            sent.append(copy)

            def put_own(cols, block, span=span):
                total[span, cols] = block.astype(bf16).astype(f32)

            product(to_x * CORES + core, s, put_own)
            copy.wait_recv()
            summed = total[span, :] + pair_in[k, span, :].astype(f32)
            if k == 0:
                total[span, :] = summed
            else:
                x_out[k - 1, span, :] = summed.astype(bf16)
                copy = remote(
                    x_out.at[k - 1, span], x_in.at[k - 1, span],
                    x_send.at[k, s], x_recv.at[k, s], {"tp": peers[k]},
                )
                copy.start()
                sent.append(copy)
                landing.append((s, copy))
    ring.pump_to(PUMP_REDUCED)

    def block(device, s):
        start = pl.multiple_of(HALO + device * rows + s * step, HALO)
        return normed_ref.at[pl.ds(start, step)]

    for s in range(pieces):
        span = pl.ds(s * step, step)
        for at, copy in landing:
            if at == s:
                copy.wait_recv()
        summed = total[span, :]
        for k in range(1, xs):
            summed = summed + x_in[k - 1, span, :].astype(f32)
        mixer_out = summed.astype(bf16).astype(f32)
        after = residual_ref[span, :].astype(f32) + rms_gain(mixer_out, cell_gain_ref[...])
        after = after.astype(bf16)
        after_ref[span, :] = after
        normed = rms_gain(after.astype(f32), ffn_gain_ref[...])
        start = pl.multiple_of(HALO + me * rows + s * step, HALO)
        normed_ref[pl.ds(start, step), :] = normed.astype(bf16)
        own = block(me, s)
        for k in range(1, xs):
            sent.append(remote(own, own, gx_send.at[k, s], gx_recv.at[k, s], {"tp": peers[k]}))
            sent[-1].start()
        sent.append(remote(own, own, gp_send.at[0, s], gp_recv.at[0, s], {"tp": partner}))
        sent[-1].start()
        ring.pump_to(PUMP_NORM[s])
    for s in range(pieces):
        for k in range(1, xs):
            came = block(sources[k], s)
            remote(came, came, gx_send.at[k, s], gx_recv.at[k, s], {"tp": peers[k]}).wait_recv()
            sent.append(remote(came, came, gp_send.at[k, s], gp_recv.at[k, s], {"tp": partner}))
            sent[-1].start()
        ring.pump_to(PUMP_GATHER[s])
    for s in range(pieces):
        for k in range(xs):
            came = block(sources[k] + partner - me, s)
            remote(came, came, gp_send.at[k, s], gp_recv.at[k, s], {"tp": partner}).wait_recv()

    ahead, behind = lax.rem(sp + 1, sps), lax.rem(sp + sps - 1, sps)
    tail = normed_ref.at[pl.ds(tok_rows, HALO)]
    head = normed_ref.at[pl.ds(0, HALO)]

    @pl.when(sp + 1 < sps)
    def _():
        remote(tail, head, h_sems.at[0], h_sems.at[1], {"sp": ahead}).start()

    @pl.when(sp == 0)
    def _():
        normed_ref[pl.ds(0, HALO), :] = jnp.zeros((HALO, width), bf16)

    ring.pump_to(PUMP_UP)
    own_up.wait()
    ring.arrived_all("up")

    @pl.when(sp > 0)
    def _():
        remote(tail, head, h_sems.at[0], h_sems.at[1], {"sp": behind}).wait_recv()

    tiles, half = up_own.shape[0], up_own.shape[2] // 2

    def up_tile(j, cols):
        lift_ref[...] = mm(normed_ref[...], up_all[j]).astype(bf16).astype(f32)
        sums = []
        for taps, side in ((gate_taps_ref, 0), (value_taps_ref, 1)):
            summed = jnp.zeros((tok_rows, half), f32)
            for offset in range(WIDTH):
                tap = taps[offset : offset + 1, cols].astype(f32)
                at = pl.ds(HALO - WIDTH + 1 + offset, tok_rows)
                summed = summed + tap * lift_ref[at, pl.ds(side * half, half)]
            sums.append(summed)
        active_ref[:, cols] = (jax.nn.gelu(sums[0], approximate=True) * sums[1]).astype(bf16)

    if half % LANES == 0:
        edges = [tiles * i // len(PUMP_TILES) for i in range(len(PUMP_TILES) + 1)]
        for i, number in enumerate(PUMP_TILES):

            @pl.loop(edges[i], edges[i + 1])
            def _(j):
                up_tile(j, pl.ds(pl.multiple_of(j * half, half), half))

            ring.pump_to(number)
    else:
        for j in range(tiles):
            up_tile(j, pl.ds(j * half, half))

    own_down.wait()

    def close_columns(shard, slot):
        copies = []
        weight = down_all[shard]
        order = list(range(1, xs)) + [0]
        for k in order:
            chunk = lax.rem(at_x + k, xs) * CORES + 1 - core
            left = active_ref[pl.ds(pl.multiple_of(chunk * rows, rows), rows), :]
            pair_out2[shard, k] = mm(left, weight).astype(bf16)
            copy = remote(
                pair_out2.at[shard, k], pair_in2.at[shard, k],
                p2_send.at[slot, k], p2_recv.at[slot, k], {"tp": partner},
            )
            copy.start()
            copies.append(copy)
        for at, k in enumerate(order):
            chunk = lax.rem(at_x + k, xs) * CORES + core
            left = active_ref[pl.ds(pl.multiple_of(chunk * rows, rows), rows), :]
            part = mm(left, weight).astype(bf16).astype(f32)
            copies[at].wait_recv()
            summed = part + pair_in2[shard, k].astype(f32)
            if k == 0:
                total2[shard] = summed
            else:
                x_out2[shard, k - 1] = summed.astype(bf16)
                copy = remote(
                    x_out2.at[shard, k - 1], x_in2.at[shard, k - 1],
                    x2_send.at[slot, k], x2_recv.at[slot, k], {"tp": peers[k]},
                )
                copy.start()
                final.append(copy)
        sent.extend(copies)

    final = []
    close_columns(sp, 0)
    slot = 1
    for hop in range(1, sps // 2 + 1):
        for way in range(2):
            if hop == sps // 2 and way == 1:
                continue
            for event in ring.events[way]:
                if event[0] == "down" and event[3] == hop:
                    ring.arrived(way, event)
            if hop == sps // 2:
                for event in ring.events[1]:
                    if event[0] == "down" and event[3] == hop:
                        ring.arrived(1, event)
            if way == 0 or hop == sps // 2:
                ring.pump(1)
            close_columns(ring.shard(way, hop), slot)
            slot += 1
            ring.pump(1)
    ring.pump(len(ring.events[0]))
    for copy in final:
        copy.wait_recv()
    square = jnp.zeros((rows, 1), f32)
    for n in range(sps):
        summed = total2[n]
        for k in range(1, xs):
            summed = summed + x_in2[n, k - 1].astype(f32)
        summed = summed.astype(bf16).astype(f32)
        total2[n] = summed
        square = square + jnp.sum(summed * summed, axis=-1, keepdims=True)
    scale = rms_scale(square, width)
    part = width // sps
    for n in range(sps):
        cols = slice(n * part, (n + 1) * part)
        result = after_ref[:, cols].astype(f32) + total2[n] * scale * close_gain_ref[:, cols]
        out_ref[:, cols] = result.astype(bf16)
    for copy in sent + final + ring.sent:
        copy.wait_send()
    for d in range(1, sps):

        @pl.when(sp + d < sps)
        def _(d=d):
            ahead = {"sp": lax.rem(sp + d, sps)}
            remote(small_out, small_in.at[d], t_send.at[d], t_recv.at[d], ahead).wait_send()
            remote(cells_out, cells_in.at[d], s_send.at[d], s_recv.at[d], ahead).wait_send()

    @pl.when(sp + 1 < sps)
    def _():
        remote(tail, head, h_sems.at[0], h_sems.at[1], {"sp": ahead}).wait_send()


PUMP_START = 4
PUMP_STATE = 5
PUMP_MIX = 7
PUMP_REDUCED = 9
PUMP_NORM = (10, 10)
PUMP_GATHER = (11, 12)
PUMP_UP = 16
PUMP_TILES = (16, 17, 18, 19)


def ring_shards(
    queries,
    keys,
    values,
    output_gate_logits,
    log_input_gate,
    forget_gate_logits,
    extra_forget_terms,
    per_head_norm_gain,
    output_weight,
    residual,
    after_cell_norm_gain,
    feedforward_norm_gain,
    closing_norm_gain,
    gate_up_weight,
    value_up_weight,
    gate_filter_taps,
    value_filter_taps,
    down_weight,
):
    count, sps = lax.axis_size("tp"), lax.axis_size("sp")
    xs = count // CORES
    tok_rows = queries.shape[0]
    heads = log_input_gate.shape[0]
    own_depth, hidden = gate_up_weight.shape
    width = output_weight.shape[1]
    own_width = down_weight.shape[1]
    rows = tok_rows // count
    pieces = 2
    half = LANES if hidden % LANES == 0 else LANES // 2
    tiles = hidden // half
    up_own = jnp.concatenate(
        [
            gate_up_weight.reshape(own_depth, tiles, half),
            value_up_weight.reshape(own_depth, tiles, half),
        ],
        axis=2,
    ).transpose(1, 0, 2)
    events = len(ring_events(sps)[0])
    vmem = pl.BlockSpec(memory_space=pltpu.VMEM)
    hbm = pl.BlockSpec(memory_space=pl.ANY)
    dma = pltpu.SemaphoreType.DMA
    V = pltpu.VMEM
    small = -(-(heads // 2 + 2 * heads) // 8) * 8
    pairs = heads // 2
    return pl.pallas_call(
        functools.partial(step_kernel, count, sps, pieces),
        out_shape=jax.ShapeDtypeStruct(residual.shape, bf16),
        in_specs=[vmem] * 13 + [hbm, vmem, vmem, hbm],
        out_specs=vmem,
        scratch_shapes=[
            V((tiles, own_depth * sps, 2 * half), bf16),
            V((sps, hidden, own_width), bf16),
            V((8, tok_rows), f32),
            V((8, tok_rows), f32),
            V((8, tok_rows), f32),
            V((tok_rows, heads * VAL_DIM), f32),
            V((tok_rows, heads * VAL_DIM), f32),
            V((heads, LANES, 2 * LANES), f32),
            V((8, LANES), f32),
            V((pairs, LANES, LANES), f32),
            V((small, LANES), f32),
            V((sps, pairs, LANES, LANES), f32),
            V((sps, small, LANES), f32),
            V((pairs, LANES, LANES), f32),
            V((8, LANES), f32),
            V((8, LANES), f32),
            V((8, LANES), f32),
            V((2, heads, LANES, 2 * LANES), bf16),
            V((tok_rows, heads * VAL_DIM), bf16),
            V((rows, width), f32),
            V((xs, rows, width), bf16),
            V((xs, rows, width), bf16),
            V((max(xs - 1, 1), rows, width), bf16),
            V((max(xs - 1, 1), rows, width), bf16),
            V((rows, width), bf16),
            V((HALO + tok_rows, width), bf16),
            V((HALO + tok_rows, 2 * half), f32),
            V((tok_rows, hidden), bf16),
            V((sps, rows, own_width), f32),
            V((sps, xs, rows, own_width), bf16),
            V((sps, xs, rows, own_width), bf16),
            V((sps, max(xs - 1, 1), rows, own_width), bf16),
            V((sps, max(xs - 1, 1), rows, own_width), bf16),
            dma((2, events)),
            dma((2, events)),
            dma((2,)),
            dma((sps,)),
            dma((sps,)),
            dma((sps,)),
            dma((sps,)),
            dma((2,)),
        ]
        + [dma((xs, pieces))] * 8
        + [dma((sps, xs))] * 4,
        compiler_params=pltpu.CompilerParams(
            collective_id=0, has_side_effects=True, vmem_limit_bytes=VMEM_BYTES
        ),
        cost_estimate=pl.CostEstimate(
            flops=6 * tok_rows * hidden * width, bytes_accessed=3 * 10**7, transcendentals=0
        ),
        name="step",
    )(
        queries, keys, values, output_gate_logits, log_input_gate, forget_gate_logits,
        extra_forget_terms, per_head_norm_gain.reshape(1, -1), output_weight, residual,
        after_cell_norm_gain.reshape(1, -1), feedforward_norm_gain.reshape(1, -1),
        closing_norm_gain.reshape(1, -1), up_own, gate_filter_taps, value_filter_taps, down_weight,
    )


class Line:
    def __init__(self, rows_z, up_own, up_all, down_own, down_all, y_send, y_recv, send, recv):
        self.rows_z = rows_z
        self.up_own, self.up_all = up_own, up_all
        self.down_own, self.down_all = down_own, down_all
        self.y_send, self.y_recv, self.send, self.recv = y_send, y_recv, send, recv
        self.sp = lax.axis_index("sp")
        self.z, self.y = self.sp // 2, lax.rem(self.sp, 2)
        self.units = [("up", yy, r) for yy in range(2) for r in range(2)]
        self.units += [("down", yy, 0) for yy in range(2)]
        self.events = [
            (unit, hop)
            for kind in ("up", "down")
            for hop in range(1, rows_z)
            for unit in self.units
            if unit[0] == kind
        ]
        self.waited = set()
        self.next = 0

    def piece(self, unit, z, y):
        kind, _, r = unit
        shard = z * 2 + y
        if kind == "down":
            return self.down_all.at[shard]
        rows = self.up_own.shape[1]
        start = pl.multiple_of(shard * rows + r * (rows // 2), rows // 2)
        return self.up_all.at[pl.ds(start, rows // 2)]

    def own(self, unit, y):
        kind, _, r = unit
        if kind == "down":
            rows = self.down_all.shape[1]
            return self.down_own.at[pl.ds(pl.multiple_of(y * rows, rows), rows)]
        rows = self.up_own.shape[1]
        return self.up_own.at[y, pl.ds(r * (rows // 2), rows // 2)]

    def side(self, yy):
        return self.y if yy == 0 else 1 - self.y

    def across(self, unit):
        at = self.units.index(("down" if unit[0] == "down" else "up", 1, unit[2]))
        return remote(
            self.own(unit, 1 - self.y), self.piece(unit, self.z, self.y),
            self.y_send.at[at], self.y_recv.at[at], {"sp": self.z * 2 + 1 - self.y},
        )

    def start_across(self):
        for unit in self.units:
            if unit[1] == 1:
                self.across(unit).start()

    def came_across(self, unit):
        if unit in self.waited:
            return
        self.waited.add(unit)
        at = self.units.index(unit)
        came = self.piece(unit, self.z, 1 - self.y)
        remote(
            came, came, self.y_send.at[at], self.y_recv.at[at], {"sp": self.z * 2 + 1 - self.y}
        ).wait_recv()

    def valid(self, way, hop):
        return self.z - hop >= 0 if way == 0 else self.z + hop < self.rows_z

    def origin(self, way, hop):
        return self.z - hop if way == 0 else self.z + hop

    def onward(self, way):
        return lax.rem(self.z + (1 if way == 0 else self.rows_z - 1), self.rows_z)

    def sends(self, way, hop):
        onward = self.z + 1 < self.rows_z if way == 0 else self.z >= 1
        return jnp.logical_and(onward, self.valid(way, hop - 1))

    def copy(self, way, event):
        unit, hop = event
        at = self.events.index(event)
        y = self.side(unit[1])
        dst = self.piece(unit, self.origin(way, hop - 1), y)
        src = self.own(unit, self.y) if hop == 1 and unit[1] == 0 else dst
        target = {"sp": self.onward(way) * 2 + self.y}
        return remote(src, dst, self.send.at[way, at], self.recv.at[way, at], target)

    def arrived(self, way, event):
        if (way, event) in self.waited:
            return
        self.waited.add((way, event))
        unit, hop = event
        at = self.events.index(event)

        @pl.when(self.valid(way, hop))
        def _():
            came = self.piece(unit, self.origin(way, hop), self.side(unit[1]))
            where = {"sp": self.onward(1 - way) * 2 + self.y}
            remote(came, came, self.send.at[way, at], self.recv.at[way, at], where).wait_recv()

    def pump_to(self, number):
        while self.next < min(number, len(self.events)):
            event = self.events[self.next]
            unit, hop = event
            if hop == 1 and unit[1] == 1:
                self.came_across(unit)
            for way in range(2):
                if hop > 1:
                    self.arrived(way, (unit, hop - 1))

                @pl.when(self.sends(way, hop))
                def _(way=way, event=event):
                    self.copy(way, event).start()

            self.next += 1

    def arrived_all(self, kind):
        for unit in self.units:
            if unit[0] == kind and unit[1] == 1:
                self.came_across(unit)
        for event in self.events:
            if event[0][0] == kind:
                for way in range(2):
                    self.arrived(way, event)

    def wait_sends(self):
        for unit in self.units:
            if unit[1] == 1:
                self.across(unit).wait_send()
        for event in self.events:
            for way in range(2):

                @pl.when(self.sends(way, event[1]))
                def _(way=way, event=event):
                    self.copy(way, event).wait_send()


def clear_state(in_cells, in_norm, in_top, in_after):
    in_cells[...] = jnp.zeros_like(in_cells)
    in_norm[...] = jnp.zeros_like(in_norm)
    in_top[...] = jnp.full_like(in_top, empty_log)
    in_after[...] = jnp.zeros_like(in_after)


def total_square(array):
    return jnp.sum(jnp.sum(array * array, axis=2, keepdims=True), axis=0, keepdims=True)


def plane_kernel(
    count, sps, pieces,
    q_ref, k_ref, v_ref, out_gate_ref, in_gate_ref, forget_ref, extra_ref, head_gain_ref,
    out_weight_ref, residual_ref, cell_gain_ref, ffn_gain_ref, close_gain_ref,
    up_own, gate_taps_ref, value_taps_ref, down_own,
    out_ref,
    up_all, down_all,
    reach_ref, top_ref, cum_ref, num_ref, den_ref, state_ref, held_ref,
    y_cells, y_small, z_cells, z_small, p_cells, p_small,
    in_cells, in_norm, in_top, in_after, enter_ref,
    mixed_ref, total, pair_out, pair_in, one_out, one_in, two_out, two_in,
    after_ref, normed_ref, lift_ref, active_ref,
    wy_send, wy_recv, wz_send, wz_recv, own_sems,
    sy_send, sy_recv, sz_send, sz_recv, h_sems,
    pair_send, pair_recv, x_send, x_recv,
    ax_send, ax_recv, ay_send, ay_recv, ad_send, ad_recv, gp_send, gp_recv,
    p2_send, p2_recv, one_send, one_recv, two_send, two_recv,
):
    sp = lax.axis_index("sp")
    me = lax.axis_index("tp")
    z, y = sp // 2, lax.rem(sp, 2)
    x, core = me // CORES, lax.rem(me, CORES)
    rows_z = sps // 2
    partner, x_peer = {"tp": x * CORES + 1 - core}, {"tp": (1 - x) * CORES + core}
    y_peer = {"sp": z * 2 + 1 - y}
    tok_rows, heads = q_ref.shape[0], in_gate_ref.shape[0]
    blocks = tok_rows // CHUNK
    rows = tok_rows // count
    step = rows // pieces
    width = out_weight_ref.shape[1]
    cw = width // sps
    pairs = heads // 2
    line = Line(
        rows_z, up_own, up_all, down_own, down_all, wy_send, wy_recv, wz_send, wz_recv
    )

    barrier = pltpu.get_barrier_semaphore()
    friends = [partner, x_peer, y_peer]
    friends += [{"sp": lax.rem(z + d, rows_z) * 2 + y} for d in range(1, rows_z)]
    for where in friends:
        pl.semaphore_signal(barrier, inc=1, device_id=where, device_id_type=MESH)
    pl.semaphore_wait(barrier, len(friends))

    line.start_across()
    line.pump_to(LINE_START)
    own_rows = up_own.shape[1]
    own_up = pltpu.make_async_copy(
        up_own.at[y],
        up_all.at[pl.ds(pl.multiple_of(sp * own_rows, own_rows), own_rows)],
        own_sems.at[0],
    )
    own_up.start()
    own_down = pltpu.make_async_copy(
        line.own(("down", 0, 0), y), down_all.at[sp], own_sems.at[1]
    )
    own_down.start()

    gate_rows_into(heads, in_gate_ref, forget_ref, extra_ref, reach_ref, top_ref, cum_ref)
    state_ref[...] = jnp.zeros_like(state_ref)
    held_ref[...] = jnp.full_like(held_ref, empty_log)

    @pl.loop(0, blocks)
    def _(b):
        cell_block(
            heads, b, q_ref, k_ref, v_ref, reach_ref, top_ref, num_ref, den_ref, state_ref, held_ref
        )

    last = cum_ref[:, pl.ds(tok_rows - LANES, LANES)]
    cum_last = jnp.broadcast_to(last[:, LANES - 1 :], last.shape)
    pack_state(heads, state_ref, held_ref, cum_last, y_cells.at[y], y_small.at[y])

    def swap(array, side, at):
        return remote(array.at[side], array.at[side], sy_send.at[at], sy_recv.at[at], y_peer)

    swap(y_small, y, 0).start()
    swap(y_cells, y, 1).start()
    swap(y_small, 1 - y, 0).wait_recv()
    swap(y_cells, 1 - y, 1).wait_recv()
    acc = (in_cells, in_norm, in_top, in_after)
    clear_state(*acc)
    merge_state(heads, y_cells.at[1], y_small.at[1], *acc)
    merge_state(heads, y_cells.at[0], y_small.at[0], *acc)
    p_cells[...] = in_cells[...]
    p_small[...] = jnp.concatenate(
        [
            in_norm[0:pairs, :], in_top[0:heads, :], in_after[0:heads, :],
            jnp.zeros((p_small.shape[0] - pairs - 2 * heads, LANES), f32),
        ],
        axis=0,
    )

    def along(d):
        where = {"sp": lax.rem(z + d, rows_z) * 2 + y}
        return (
            remote(p_small, z_small.at[d], sz_send.at[0, d], sz_recv.at[0, d], where),
            remote(p_cells, z_cells.at[d], sz_send.at[1, d], sz_recv.at[1, d], where),
        )

    for d in range(1, rows_z):

        @pl.when(z + d < rows_z)
        def _(d=d):
            for copy in along(d):
                copy.start()

    line.pump_to(LINE_STATE)
    clear_state(*acc)

    @pl.when(y == 1)
    def _():
        merge_state(heads, y_cells.at[0], y_small.at[0], *acc)

    for d in range(1, rows_z):

        @pl.when(z - d >= 0)
        def _(d=d):
            for copy in along(d):
                copy.wait_recv()
            merge_state(heads, z_cells.at[d], z_small.at[d], *acc)

    for pair in range(pairs):
        norm = jnp.broadcast_to(in_norm[pair : pair + 1, :], (LANES, LANES)).T
        full = jnp.concatenate([in_cells[pair], norm], axis=1)
        row = lax.broadcasted_iota(jnp.int32, full.shape, 0)
        for h in (2 * pair, 2 * pair + 1):
            own = (row >= KEY_DIM) if h % 2 else (row < KEY_DIM)
            high, low = split(jnp.where(own, full, 0.0))
            enter_ref[0, h] = high
            enter_ref[1, h] = low
    line.pump_to(LINE_MIX)

    @pl.loop(0, blocks)
    def _(b):
        mix_block(
            heads, b, q_ref, out_gate_ref, head_gain_ref, top_ref, cum_ref, num_ref, den_ref,
            in_top, enter_ref, mixed_ref,
        )

    def product(chunk, piece, store):
        start = pl.multiple_of(chunk * rows + piece * step, step)
        left = mixed_ref[pl.ds(start, step), :]

        @pl.loop(0, sps)
        def _(j):
            cols = pl.ds(pl.multiple_of(j * cw, cw), cw)
            store(j, mm(left, out_weight_ref[:, cols]))

    sent, landing = [], []
    for k in (1, 0):
        to_x = x if k == 0 else 1 - x
        for s in range(pieces):
            span = pl.ds(s * step, step)

            def put_pair(j, block, k=k, span=span):
                pair_out[j, k, span, :] = block.astype(bf16)

            product(to_x * CORES + 1 - core, s, put_pair)
            copy = remote(
                pair_out.at[:, k, span], pair_in.at[:, k, span],
                pair_send.at[k, s], pair_recv.at[k, s], partner,
            )
            copy.start()
            sent.append(copy)

            def put_own(j, block, span=span):
                total[j, span, :] = block.astype(bf16).astype(f32)

            product(to_x * CORES + core, s, put_own)
            copy.wait_recv()
            summed = total[:, span, :] + pair_in[:, k, span, :].astype(f32)
            if k == 0:
                total[:, span, :] = summed
            else:
                one_out[:, s] = summed.astype(bf16)
                copy = remote(
                    one_out.at[:, s], one_in.at[:, s], x_send.at[s], x_recv.at[s], x_peer
                )
                copy.start()
                sent.append(copy)
                landing.append(copy)
    line.pump_to(LINE_REDUCED)

    def block(side, owner, s):
        start = pl.multiple_of(HALO + side * tok_rows + owner * rows + s * step, HALO)
        return normed_ref.at[pl.ds(start, step)]

    def give(array, sems, at, where):
        copy = remote(array, array, sems[0].at[at], sems[1].at[at], where)
        copy.start()
        sent.append(copy)

    def take(array, sems, at, where):
        remote(array, array, sems[0].at[at], sems[1].at[at], where).wait_recv()

    to_x, to_y, to_d = (ax_send, ax_recv), (ay_send, ay_recv), (ad_send, ad_recv)
    to_p = (gp_send, gp_recv)
    other = (1 - x) * CORES + core
    for s in range(pieces):
        span = pl.ds(s * step, step)
        landing[s].wait_recv()
        summed = total[:, span, :] + one_in[:, s].astype(f32)
        mixer_out = summed.astype(bf16).astype(f32)
        scale = rms_scale(total_square(mixer_out), width)
        held = []
        for j in range(sps):
            cols = slice(j * cw, (j + 1) * cw)
            after = residual_ref[span, cols].astype(f32) + (
                mixer_out[j] * scale[0] * cell_gain_ref[:, cols]
            )
            after = after.astype(bf16)
            after_ref[j, span, :] = after
            held.append(after.astype(f32))
        square = sum(jnp.sum(a * a, axis=-1, keepdims=True) for a in held)
        scale = rms_scale(square, width)
        start = pl.multiple_of(HALO + y * tok_rows + me * rows + s * step, HALO)
        for j in range(sps):
            cols = slice(j * cw, (j + 1) * cw)
            normed_ref[pl.ds(start, step), cols] = (
                held[j] * scale * ffn_gain_ref[:, cols]
            ).astype(bf16)
        own = block(y, me, s)
        give(own, to_y, s, y_peer)
        give(own, to_x, s, x_peer)
        give(own, to_p, s, partner)
        line.pump_to(LINE_NORM[s])
    for s in range(pieces):
        from_x, from_y = block(y, other, s), block(1 - y, me, s)
        if s == 0:
            take(from_y, to_y, s, y_peer)
            give(from_y, to_d, s, x_peer)
            give(from_y, to_p, 2 * pieces + s, partner)
            take(from_x, to_x, s, x_peer)
            give(from_x, to_p, pieces + s, partner)
        else:
            take(from_x, to_x, s, x_peer)
            give(from_x, to_d, s, y_peer)
            give(from_x, to_p, pieces + s, partner)
            take(from_y, to_y, s, y_peer)
            give(from_y, to_p, 2 * pieces + s, partner)
        line.pump_to(LINE_GATHER[s])
    for s in range(pieces):
        from_d = block(1 - y, other, s)
        take(from_d, to_d, s, x_peer if s == 0 else y_peer)
        give(from_d, to_p, 3 * pieces + s, partner)
    mate, other_mate = x * CORES + 1 - core, (1 - x) * CORES + 1 - core
    for s in range(pieces):
        take(block(y, mate, s), to_p, s, partner)
        take(block(y, other_mate, s), to_p, pieces + s, partner)
        take(block(1 - y, mate, s), to_p, 2 * pieces + s, partner)
        take(block(1 - y, other_mate, s), to_p, 3 * pieces + s, partner)

    group = 2 * tok_rows

    def halo(plane):
        return remote(
            normed_ref.at[pl.ds(group, HALO)], normed_ref.at[pl.ds(0, HALO)],
            h_sems.at[0], h_sems.at[1], {"sp": lax.rem(plane, rows_z) * 2 + y},
        )

    @pl.when(z + 1 < rows_z)
    def _():
        halo(z + 1).start()

    @pl.when(z == 0)
    def _():
        normed_ref[pl.ds(0, HALO), :] = jnp.zeros((HALO, width), bf16)

    line.pump_to(LINE_UP)
    own_up.wait()
    line.arrived_all("up")

    @pl.when(z > 0)
    def _():
        halo(z + rows_z - 1).wait_recv()

    hidden = active_ref.shape[1]
    full, rest = hidden // LANES, hidden % LANES

    def up_tile(weight_cols, cols, half):
        lift_ref[:, pl.ds(0, 2 * half)] = (
            mm(normed_ref[...], up_all[:, weight_cols]).astype(bf16).astype(f32)
        )

        @pl.loop(0, group // CONV_ROWS)
        def _(i):
            sums = []
            for taps, side in ((gate_taps_ref, 0), (value_taps_ref, 1)):
                summed = jnp.zeros((CONV_ROWS, half), f32)
                base = pl.multiple_of(i * CONV_ROWS, CONV_ROWS)
                window = lift_ref[pl.ds(base, CONV_ROWS + HALO), pl.ds(side * half, half)]
                for offset in range(WIDTH):
                    tap = taps[y, offset : offset + 1, cols].astype(f32)
                    low = HALO - WIDTH + 1 + offset
                    summed = summed + tap * window[low : low + CONV_ROWS]
                sums.append(summed)
            active = jax.nn.gelu(sums[0], approximate=True) * sums[1]
            active_ref[pl.ds(base, CONV_ROWS), cols] = active.astype(bf16)

    edges = [full * i // len(LINE_TILES) for i in range(len(LINE_TILES) + 1)]
    for i, number in enumerate(LINE_TILES):

        @pl.loop(edges[i], edges[i + 1])
        def _(j):
            up_tile(
                pl.ds(pl.multiple_of(j * 2 * LANES, 2 * LANES), 2 * LANES),
                pl.ds(pl.multiple_of(j * LANES, LANES), LANES),
                LANES,
            )

        line.pump_to(number)
    if rest:
        up_tile(pl.ds(full * 2 * LANES, 2 * rest), pl.ds(full * LANES, rest), rest)

    own_down.wait()
    for copy in sent:
        copy.wait_send()

    def chunk_rows(side, at_x, at_core):
        start = side * tok_rows + (at_x * CORES + at_core) * rows
        return pl.ds(pl.multiple_of(start, rows), rows)

    sides = ((1 - y, 1 - x), (y, 1 - x), (1 - y, x), (y, x))

    def pair_copy(shard, k):
        return remote(
            pair_out.at[shard, k], pair_in.at[shard, k],
            p2_send.at[shard, k], p2_recv.at[shard, k], partner,
        )

    def one_copy(shard, at):
        return remote(
            one_out.at[shard, at], one_in.at[shard, at],
            one_send.at[shard, at], one_recv.at[shard, at], x_peer if at < 2 else y_peer,
        )

    def two_copy(shard, at):
        return remote(
            two_out.at[shard, at], two_in.at[shard, at],
            two_send.at[shard, at], two_recv.at[shard, at], y_peer if at == 0 else x_peer,
        )

    low, high = slice(0, step), slice(step, rows)

    def multiply(shard):
        weight = down_all[shard]
        for k, (side, at_x) in enumerate(sides):
            left = active_ref[chunk_rows(side, at_x, 1 - core), :]
            pair_out[shard, k] = mm(left, weight).astype(bf16)
            pair_copy(shard, k).start()
        for k, (side, at_x) in enumerate(sides):
            left = active_ref[chunk_rows(side, at_x, core), :]
            part = mm(left, weight).astype(bf16).astype(f32)
            pair_copy(shard, k).wait_recv()
            summed = part + pair_in[shard, k].astype(f32)
            if k == 0:
                one_out[shard, 0] = summed[low].astype(bf16)
                one_copy(shard, 0).start()
                one_out[shard, 2] = summed[high].astype(bf16)
                one_copy(shard, 2).start()
            elif k == 1:
                one_out[shard, 1] = summed[low].astype(bf16)
                one_copy(shard, 1).start()
                two_out[shard, 1] = summed[high].astype(bf16)
            elif k == 2:
                one_out[shard, 3] = summed[high].astype(bf16)
                one_copy(shard, 3).start()
                two_out[shard, 0] = summed[low].astype(bf16)
            else:
                total[shard] = summed

    def pass_on(shard):
        one_copy(shard, 0).wait_recv()
        summed = two_out[shard, 0].astype(f32) + one_in[shard, 0].astype(f32)
        two_out[shard, 0] = summed.astype(bf16)
        two_copy(shard, 0).start()
        one_copy(shard, 2).wait_recv()
        summed = two_out[shard, 1].astype(f32) + one_in[shard, 2].astype(f32)
        two_out[shard, 1] = summed.astype(bf16)
        two_copy(shard, 1).start()
        one_copy(shard, 1).wait_recv()
        one_copy(shard, 3).wait_recv()

    steps = [(None, 0, 0), (None, 0, 1)]
    for hop in range(1, rows_z):
        for yy in range(2):
            for way in range(2):
                steps.append((way, hop, yy))

    def shard_of(way, hop, yy):
        return (z if way is None else line.origin(way, hop)) * 2 + line.side(yy)

    def at_step(entry, action):
        way, hop, yy = entry
        if way is None:
            action()
        else:
            pl.when(line.valid(way, hop))(action)

    first_down = 4 * (rows_z - 1)
    waiting = []
    for way, hop, yy in steps:
        unit = ("down", yy, 0)
        if way is None:
            if yy:
                line.came_across(unit)
        else:
            line.pump_to(first_down + 2 * hop + yy + 1)
            line.arrived(way, (unit, hop))
        entry = (way, hop, yy)
        shard = shard_of(way, hop, yy)
        at_step(entry, functools.partial(multiply, shard))
        waiting.append((entry, shard))
        if len(waiting) > 2:
            entry, shard = waiting.pop(0)
            at_step(entry, functools.partial(pass_on, shard))
    for entry, shard in waiting:
        at_step(entry, functools.partial(pass_on, shard))
    for entry in steps:

        def finish(entry=entry):
            shard = shard_of(*entry)
            two_copy(shard, 0).wait_recv()
            two_copy(shard, 1).wait_recv()
            total[shard, low] = (
                total[shard, low] + one_in[shard, 1].astype(f32) + two_in[shard, 0].astype(f32)
            )
            total[shard, high] = (
                total[shard, high] + one_in[shard, 3].astype(f32) + two_in[shard, 1].astype(f32)
            )

        at_step(entry, finish)
    summed = total[...].astype(bf16).astype(f32)
    scale = rms_scale(total_square(summed), width)
    for j in range(sps):
        cols = slice(j * cw, (j + 1) * cw)
        result = after_ref[j].astype(f32) + summed[j] * scale[0] * close_gain_ref[:, cols]
        out_ref[:, cols] = result.astype(bf16)

    for entry in steps:

        def sends_done(entry=entry):
            shard = shard_of(*entry)
            for k in range(4):
                pair_copy(shard, k).wait_send()
                one_copy(shard, k).wait_send()
            for k in range(2):
                two_copy(shard, k).wait_send()

        at_step(entry, sends_done)
    line.wait_sends()
    swap(y_small, y, 0).wait_send()
    swap(y_cells, y, 1).wait_send()
    for d in range(1, rows_z):

        @pl.when(z + d < rows_z)
        def _(d=d):
            for copy in along(d):
                copy.wait_send()

    @pl.when(z + 1 < rows_z)
    def _():
        halo(z + 1).wait_send()


LINE_START = 2
LINE_STATE = 4
LINE_MIX = 6
LINE_REDUCED = 9
LINE_NORM = (10, 10)
LINE_GATHER = (11, 12)
LINE_UP = 14
LINE_TILES = (14, 14)
CONV_ROWS = 256


def by_side(array, axis):
    shape = array.shape
    parted = shape[:axis] + (2, shape[axis] // 2) + shape[axis + 1 :]
    return jnp.moveaxis(array.reshape(parted), axis, 0)


def plane_shards(
    queries, keys, values, output_gate_logits, log_input_gate, forget_gate_logits,
    extra_forget_terms, per_head_norm_gain, output_weight, residual, after_cell_norm_gain,
    feedforward_norm_gain, closing_norm_gain, gate_up_weight, value_up_weight,
    gate_filter_taps, value_filter_taps, down_weight,
):
    count, sps = lax.axis_size("tp"), lax.axis_size("sp")
    rows_z = sps // 2
    tok_rows = queries.shape[0]
    heads = log_input_gate.shape[0]
    own_depth = gate_up_weight.shape[0]
    hidden = gate_up_weight.shape[1] // 2
    width = output_weight.shape[1]
    cw = down_weight.shape[1]
    rows = tok_rows // count
    pieces = 2
    step = rows // pieces
    gate_parts, value_parts = by_side(gate_up_weight, 1), by_side(value_up_weight, 1)
    tiles = []
    for start in range(0, hidden, LANES):
        cols = slice(start, min(start + LANES, hidden))
        tiles += [gate_parts[:, :, cols], value_parts[:, :, cols]]
    up_own = jnp.concatenate(tiles, axis=2)
    vmem = pl.BlockSpec(memory_space=pltpu.VMEM)
    hbm = pl.BlockSpec(memory_space=pl.ANY)
    dma = pltpu.SemaphoreType.DMA
    V = pltpu.VMEM
    pairs = heads // 2
    small = -(-(pairs + 2 * heads) // 8) * 8
    cells = (pairs, LANES, LANES)
    return pl.pallas_call(
        functools.partial(plane_kernel, count, sps, pieces),
        out_shape=jax.ShapeDtypeStruct(residual.shape, bf16),
        in_specs=[vmem] * 13 + [hbm, vmem, vmem, hbm],
        out_specs=vmem,
        scratch_shapes=[
            V((own_depth * sps, 2 * hidden), bf16),
            V((sps, hidden, cw), bf16),
            V((8, tok_rows), f32),
            V((8, tok_rows), f32),
            V((8, tok_rows), f32),
            V((tok_rows, heads * VAL_DIM), f32),
            V((tok_rows, heads * VAL_DIM), f32),
            V((heads, LANES, 2 * LANES), f32),
            V((8, LANES), f32),
            V((2,) + cells, f32),
            V((2, small, LANES), f32),
            V((rows_z,) + cells, f32),
            V((rows_z, small, LANES), f32),
            V(cells, f32),
            V((small, LANES), f32),
            V(cells, f32),
            V((8, LANES), f32),
            V((8, LANES), f32),
            V((8, LANES), f32),
            V((2, heads, LANES, 2 * LANES), bf16),
            V((tok_rows, heads * VAL_DIM), bf16),
            V((sps, rows, cw), f32),
            V((sps, 4, rows, cw), bf16),
            V((sps, 4, rows, cw), bf16),
            V((sps, 4, step, cw), bf16),
            V((sps, 4, step, cw), bf16),
            V((sps, 2, step, cw), bf16),
            V((sps, 2, step, cw), bf16),
            V((sps, rows, cw), bf16),
            V((HALO + 2 * tok_rows, width), bf16),
            V((HALO + 2 * tok_rows, 2 * LANES), f32),
            V((2 * tok_rows, hidden), bf16),
            dma((6,)),
            dma((6,)),
            dma((2, 6 * (rows_z - 1))),
            dma((2, 6 * (rows_z - 1))),
            dma((2,)),
            dma((2,)),
            dma((2,)),
            dma((2, rows_z)),
            dma((2, rows_z)),
            dma((2,)),
            dma((2, pieces)),
            dma((2, pieces)),
            dma((pieces,)),
            dma((pieces,)),
        ]
        + [dma((pieces,))] * 6
        + [dma((4 * pieces,))] * 2
        + [dma((sps, 4))] * 4
        + [dma((sps, 2))] * 2,
        compiler_params=pltpu.CompilerParams(
            collective_id=0, has_side_effects=True, vmem_limit_bytes=VMEM_BYTES
        ),
        cost_estimate=pl.CostEstimate(
            flops=12 * tok_rows * hidden * width, bytes_accessed=3 * 10**7, transcendentals=0
        ),
        name="plane",
    )(
        queries, keys, values, output_gate_logits, log_input_gate, forget_gate_logits,
        extra_forget_terms, per_head_norm_gain.reshape(1, -1), output_weight, residual,
        after_cell_norm_gain.reshape(1, -1), feedforward_norm_gain.reshape(1, -1),
        closing_norm_gain.reshape(1, -1), up_own, by_side(gate_filter_taps, 1),
        by_side(value_filter_taps, 1), down_weight,
    )


def shards(*arrays):
    count, sps = lax.axis_size("tp"), lax.axis_size("sp")
    hidden, own_width = arrays[17].shape
    plane = (
        grid_of(sps)[1] == 2
        and count == 2 * CORES
        and own_width % LANES == 0
        and hidden % 32 == 0
    )
    return plane_shards(*arrays) if plane else ring_shards(*arrays)


def solution(mesh):
    placed = (
        P("sp", "tp"),
        P("sp", "tp"),
        P("sp", "tp"),
        P("sp", "tp"),
        P("tp", "sp"),
        P("tp", "sp"),
        P("tp", "sp"),
        P("tp"),
        P("tp", None),
        P(("sp", "tp"), None),
        P(),
        P(),
        P(),
        P("sp", "tp"),
        P("sp", "tp"),
        P(None, "tp"),
        P(None, "tp"),
        P("tp", "sp"),
    )
    return jax.shard_map(
        shards, mesh=mesh, in_specs=placed, out_specs=P(("sp", "tp"), None), check_vma=False
    )
```

```python
import functools

import jax
import jax.numpy as jnp
from jax import lax
from jax.experimental import pallas as pl
from jax.experimental.pallas import tpu as pltpu
from jax.sharding import PartitionSpec as P

MESH = pl.DeviceIdType.MESH
CORES = 2
KEY_DIM = 64
VAL_DIM = 128
WIDTH = 3
LANES = 128
CHUNK = 128
HALO = 16
VMEM_BYTES = 67_000_000

eps = 1e-06
empty_log = -1e30
f32, bf16 = jnp.float32, jnp.bfloat16


def rms_scale(total_square, width):
    return lax.rsqrt(total_square / width + eps)


def rms_gain(inputs, gains):
    return inputs * lax.rsqrt(jnp.mean(inputs * inputs, axis=-1, keepdims=True) + eps) * gains


def remote(src, dst, send, recv, where):
    return pltpu.make_async_remote_copy(
        src_ref=src,
        dst_ref=dst,
        send_sem=send,
        recv_sem=recv,
        device_id=where,
        device_id_type=MESH,
    )


def mm(left, right):
    return jnp.dot(left, right, preferred_element_type=f32)


def split(array):
    high = array.astype(bf16)
    return high, (array - high.astype(f32)).astype(bf16)


def scan_lanes(array, op, neutral):
    length = array.shape[1]
    lane = lax.broadcasted_iota(jnp.int32, array.shape, 1)
    shift = 1
    while shift < length:
        moved = pltpu.roll(array, shift, 1)
        array = op(array, jnp.where(lane >= shift, moved, neutral))
        shift *= 2
    return array


def grid_of(count):
    rows_y = 1
    while 8 * rows_y * rows_y <= count:
        rows_y *= 2
    return count // rows_y, rows_y


def to_sp(place, count):
    rows_z, rows_y = grid_of(count)
    at_y, k = place // rows_z, lax.rem(place, rows_z)
    at_z = jnp.where(lax.rem(at_y, 2) == 0, k, rows_z - 1 - k)
    return at_z * rows_y + at_y


def to_place(sp, count):
    rows_z, rows_y = grid_of(count)
    at_z, at_y = sp // rows_y, lax.rem(sp, rows_y)
    return at_y * rows_z + jnp.where(lax.rem(at_y, 2) == 0, at_z, rows_z - 1 - at_z)


def reach_of(count, way, half):
    return count // 2 if way == half else count // 2 - 1


def ring_events(count):
    ways = []
    for way in range(2):
        events = []
        for kind in ("up", "down"):
            for hop in range(1, count // 2 + 1):
                for half in range(2):
                    if hop <= reach_of(count, way, half):
                        for part in range(2 if kind == "up" else 1):
                            events.append((kind, half, part, hop))
        ways.append(events)
    return ways


class Ring:
    def __init__(self, count, up_own, up_all, down_own, down_all, send, recv):
        self.count = count
        self.up_own, self.up_all = up_own, up_all
        self.down_own, self.down_all = down_own, down_all
        self.send, self.recv = send, recv
        self.place = to_place(lax.axis_index("sp"), count)
        self.events = ring_events(count)
        self.at = [{e: i for i, e in enumerate(events)} for events in self.events]
        self.waited = set()
        self.sent = []
        self.next = 0

    def piece(self, kind, half, part, shard, own):
        if kind == "up":
            tiles, rows = self.up_own.shape[0], self.up_own.shape[1]
            low = (tiles + 1) // 2
            span = pl.ds(0, low) if part == 0 else pl.ds(low, tiles - low)
            if tiles == 1:
                return None if part else self._up(pl.ds(0, 1), half, shard, rows, own)
            return self._up(span, half, shard, rows, own)
        rows = self.down_own.shape[0] // 2
        span = pl.ds(half * rows, rows)
        return self.down_own.at[span] if own else self.down_all.at[shard, span]

    def _up(self, span, half, shard, rows, own):
        if own:
            return self.up_own.at[span, pl.ds(half * (rows // 2), rows // 2)]
        start = pl.multiple_of(shard * rows + half * (rows // 2), rows // 2)
        return self.up_all.at[span, pl.ds(start, rows // 2)]

    def shard(self, way, hop):
        step = hop if way == 0 else self.count - hop
        return to_sp(lax.rem(self.place + self.count - step, self.count), self.count)

    def copy(self, way, event, target):
        kind, half, part, hop = event
        at = self.at[way][event]
        shard = self.shard(way, hop - 1)
        src = self.piece(kind, half, part, shard, hop == 1)
        dst = self.piece(kind, half, part, shard, False)
        return remote(src, dst, self.send.at[way, at], self.recv.at[way, at], target)

    def arrived(self, way, event):
        if (way, event) in self.waited:
            return
        self.waited.add((way, event))
        kind, half, part, hop = event
        at = self.at[way][event]
        came = self.piece(kind, half, part, self.shard(way, hop), False)
        where = {"sp": self.shard(way, 1)}
        remote(came, came, self.send.at[way, at], self.recv.at[way, at], where).wait_recv()

    def pump(self, times=1):
        for _ in range(times):
            if self.next >= len(self.events[0]):
                return
            for way in range(2):
                event = self.events[way][self.next]
                kind, half, part, hop = event
                if hop > 1:
                    self.arrived(way, (kind, half, part, hop - 1))
                target = {"sp": self.shard(1 - way, 1)}
                copy = self.copy(way, event, target)
                copy.start()
                self.sent.append(copy)
            self.next += 1

    def pump_to(self, number):
        self.pump(max(number - self.next, 0))

    def arrived_all(self, kind, hop=None):
        for way in range(2):
            for event in self.events[way]:
                if event[0] == kind and (hop is None or event[3] == hop):
                    self.arrived(way, event)


def tp_places(count):
    me = lax.axis_index("tp")
    at_x, core = me // CORES, lax.rem(me, CORES)
    xs = count // CORES
    partner = at_x * CORES + 1 - core
    peers = [lax.rem(at_x + k, xs) * CORES + core for k in range(xs)]
    sources = [lax.rem(at_x + xs - k, xs) * CORES + core for k in range(xs)]
    return me, at_x, core, partner, peers, sources


def columns_of(rows):
    depth = rows.shape[0]
    if depth < LANES:
        rows = jnp.concatenate([rows, jnp.zeros((LANES - depth, LANES), f32)], axis=0)
    return rows.T


def column(turned, at):
    return jnp.broadcast_to(turned[:, at : at + 1], (turned.shape[0], LANES))


def wide(array):
    return jnp.concatenate([array, array], axis=1)


def gate_rows_into(heads, gate_ref, forget_ref, extra_ref, reach_ref, top_ref, cum_ref):
    def full(ref):
        array = ref[...]
        return jnp.concatenate([array] * (8 // heads), axis=0)

    logits = full(forget_ref)
    cum = scan_lanes(full(extra_ref) - jnp.log1p(jnp.exp(-logits)), jnp.add, 0.0)
    reach = full(gate_ref) - cum
    cum_ref[...] = cum
    reach_ref[...] = reach
    top_ref[...] = scan_lanes(reach, jnp.maximum, empty_log)


def cell_block(heads, b, q_ref, k_ref, v_ref, reach_ref, top_ref, num_ref, den_ref, state_ref, held_ref):
    rows = pl.ds(pl.multiple_of(b * CHUNK, CHUNK), CHUNK)
    reach, top = reach_ref[:, rows], top_ref[:, rows]
    before = held_ref[...]
    now = jnp.broadcast_to(jnp.max(top, axis=1, keepdims=True), top.shape)
    held_ref[...] = now
    turned = columns_of(jnp.concatenate([top, jnp.exp(before - top)], axis=0))
    fade = jnp.exp(before - now)
    weight = jnp.exp(reach - now)
    at_t = lax.broadcasted_iota(jnp.int32, (CHUNK, CHUNK), 0)
    at_s = lax.broadcasted_iota(jnp.int32, (CHUNK, CHUNK), 1)
    causal = at_s <= at_t
    ones = jnp.ones((CHUNK, LANES), bf16)
    for pair in range(heads // 2):
        pair_cols = pl.ds(pair * LANES, LANES)
        query = q_ref[rows, pair_cols]
        turned_keys = k_ref[rows, pair_cols].astype(f32).T
        for h in (2 * pair, 2 * pair + 1):
            cols = pl.ds(h * VAL_DIM, VAL_DIM)
            value = jnp.concatenate([v_ref[rows, cols], ones], axis=1)
            own = (at_t >= KEY_DIM) if h % 2 else (at_t < KEY_DIM)
            keys = jnp.where(own, turned_keys, 0.0)
            decay = jnp.exp(jnp.where(causal, reach[h : h + 1, :] - column(turned, h), empty_log))
            high, low = split(mm(query, keys.astype(bf16)) * decay)
            state = state_ref[h]
            state_high, state_low = split(state)
            carried = mm(query, state_high) + mm(query, state_low)
            total = mm(high, value) + mm(low, value) + wide(column(turned, 8 + h)) * carried
            num_ref[rows, cols] = total[:, :LANES]
            den_ref[rows, cols] = total[:, LANES:]
            high, low = split(keys * weight[h : h + 1, :])
            state_ref[h] = state * wide(fade[h : h + 1, :]) + mm(high, value) + mm(low, value)


def pack_state(heads, state_ref, held_ref, cum_last, cells_ref, small_ref):
    pairs = heads // 2
    rows = []
    for pair in range(pairs):
        both = state_ref[2 * pair] + state_ref[2 * pair + 1]
        cells_ref[pair] = both[:, :LANES]
        rows.append(both[:, LANES:].T[0:1, :])
    tops = held_ref[0:heads, :] + cum_last[0:heads, :]
    rows += [tops, cum_last[0:heads, :]]
    used = pairs + 2 * heads
    rows.append(jnp.zeros((small_ref.shape[0] - used, LANES), f32))
    small_ref[...] = jnp.concatenate(rows, axis=0)


def merge_state(heads, cells_ref, small_ref, in_cells, in_norm, in_top, in_after):
    pairs = heads // 2
    small = small_ref[...]
    tops, totals = small[pairs : pairs + heads, :], small[pairs + heads : pairs + 2 * heads, :]
    top, after = in_top[0:heads, :], in_after[0:heads, :]
    reach = after + tops
    best = jnp.maximum(top, reach)
    old, new = jnp.exp(top - best), jnp.exp(reach - best)
    in_top[0:heads, :] = best
    in_after[0:heads, :] = after + totals
    lane = lax.broadcasted_iota(jnp.int32, (1, LANES), 1) < KEY_DIM
    row = lax.broadcasted_iota(jnp.int32, (LANES, LANES), 0) < KEY_DIM
    for pair in range(pairs):
        a, b = slice(2 * pair, 2 * pair + 1), slice(2 * pair + 1, 2 * pair + 2)
        in_norm[pair : pair + 1, :] = (
            jnp.where(lane, old[a], old[b]) * in_norm[pair : pair + 1, :]
            + jnp.where(lane, new[a], new[b]) * small[pair : pair + 1, :]
        )
        in_cells[pair] = (
            jnp.where(row, old[a], old[b]) * in_cells[pair]
            + jnp.where(row, new[a], new[b]) * cells_ref[pair]
        )


def mix_block(
    heads, b, q_ref, gate_ref, gain_ref, top_ref, cum_ref, num_ref, den_ref, in_top, enter_ref, mixed_ref
):
    rows = pl.ds(pl.multiple_of(b * CHUNK, CHUNK), CHUNK)
    top, cum, came = top_ref[:, rows], cum_ref[:, rows], in_top[...]
    best = jnp.maximum(top, came)
    turned = columns_of(
        jnp.concatenate([jnp.exp(top - best), jnp.exp(came - best), jnp.exp(-(cum + best))], axis=0)
    )
    scale = KEY_DIM ** (-0.5)
    for pair in range(heads // 2):
        query = q_ref[rows, pl.ds(pair * LANES, LANES)]
        for h in (2 * pair, 2 * pair + 1):
            cols = pl.ds(h * VAL_DIM, VAL_DIM)
            carried = mm(query, enter_ref[0, h]) + mm(query, enter_ref[1, h])
            here, there, floor = column(turned, h), column(turned, 8 + h), column(turned, 16 + h)
            num = (here * num_ref[rows, cols] + there * carried[:, :LANES]) * scale
            den = (here * den_ref[rows, cols] + there * carried[:, LANES:]) * scale
            out = num / jnp.maximum(jnp.abs(den), floor)
            gate = jax.nn.sigmoid(gate_ref[rows, cols].astype(f32))
            mixed_ref[rows, cols] = (out * gain_ref[:, cols] * gate).astype(bf16)


def step_kernel(
    count, sps, pieces,
    q_ref, k_ref, v_ref, out_gate_ref, in_gate_ref, forget_ref, extra_ref, head_gain_ref,
    out_weight_ref, residual_ref, cell_gain_ref, ffn_gain_ref, close_gain_ref,
    up_own, gate_taps_ref, value_taps_ref, down_own,
    out_ref,
    up_all, down_all,
    reach_ref, top_ref, cum_ref, num_ref, den_ref, state_ref, held_ref,
    cells_out, small_out, cells_in, small_in, in_cells, in_norm, in_top, in_after, enter_ref,
    mixed_ref, total, pair_out, pair_in, x_out, x_in, after_ref, normed_ref, lift_ref, active_ref,
    total2, pair_out2, pair_in2, x_out2, x_in2,
    ring_send, ring_recv, own_sems, s_send, s_recv, t_send, t_recv, h_sems,
    pair_send, pair_recv, x_send, x_recv, gx_send, gx_recv, gp_send, gp_recv,
    p2_send, p2_recv, x2_send, x2_recv,
):
    sp = lax.axis_index("sp")
    me, at_x, core, partner, peers, sources = tp_places(count)
    xs = count // CORES
    tok_rows, heads = q_ref.shape[0], in_gate_ref.shape[0]
    blocks = tok_rows // CHUNK
    rows = tok_rows // count
    step = rows // pieces
    width = out_weight_ref.shape[1]
    ring = Ring(sps, up_own, up_all, down_own, down_all, ring_send, ring_recv)

    barrier = pltpu.get_barrier_semaphore()
    for d in range(1, sps):
        pl.semaphore_signal(
            barrier, inc=1, device_id={"sp": lax.rem(sp + d, sps)}, device_id_type=MESH
        )
    for where in [partner] + peers[1:]:
        pl.semaphore_signal(barrier, inc=1, device_id={"tp": where}, device_id_type=MESH)
    pl.semaphore_wait(barrier, sps - 1 + xs)

    ring.pump_to(PUMP_START)
    own_rows = up_own.shape[1]
    own_up = pltpu.make_async_copy(
        up_own,
        up_all.at[:, pl.ds(pl.multiple_of(sp * own_rows, own_rows), own_rows)],
        own_sems.at[0],
    )
    own_up.start()
    own_down = pltpu.make_async_copy(down_own, down_all.at[sp], own_sems.at[1])
    own_down.start()

    gate_rows_into(heads, in_gate_ref, forget_ref, extra_ref, reach_ref, top_ref, cum_ref)
    state_ref[...] = jnp.zeros_like(state_ref)
    held_ref[...] = jnp.full_like(held_ref, empty_log)

    @pl.loop(0, blocks)
    def _(b):
        cell_block(
            heads, b, q_ref, k_ref, v_ref, reach_ref, top_ref, num_ref, den_ref, state_ref, held_ref
        )

    last = cum_ref[:, pl.ds(tok_rows - LANES, LANES)]
    cum_last = jnp.broadcast_to(last[:, LANES - 1 :], last.shape)
    pack_state(heads, state_ref, held_ref, cum_last, cells_out, small_out)
    for d in range(1, sps):
        ahead = {"sp": lax.rem(sp + d, sps)}

        @pl.when(sp + d < sps)
        def _(d=d, ahead=ahead):
            remote(small_out, small_in.at[d], t_send.at[d], t_recv.at[d], ahead).start()
            remote(cells_out, cells_in.at[d], s_send.at[d], s_recv.at[d], ahead).start()

    ring.pump_to(PUMP_STATE)
    in_cells[...] = jnp.zeros_like(in_cells)
    in_norm[...] = jnp.zeros_like(in_norm)
    in_top[...] = jnp.full_like(in_top, empty_log)
    in_after[...] = jnp.zeros_like(in_after)
    for d in range(1, sps):

        @pl.when(sp - d >= 0)
        def _(d=d):
            behind = {"sp": lax.rem(sp + sps - d, sps)}
            remote(small_out, small_in.at[d], t_send.at[d], t_recv.at[d], behind).wait_recv()
            remote(cells_out, cells_in.at[d], s_send.at[d], s_recv.at[d], behind).wait_recv()
            merge_state(
                heads, cells_in.at[d], small_in.at[d], in_cells, in_norm, in_top, in_after
            )

    for pair in range(heads // 2):
        norm = jnp.broadcast_to(in_norm[pair : pair + 1, :], (LANES, LANES)).T
        full = jnp.concatenate([in_cells[pair], norm], axis=1)
        row = lax.broadcasted_iota(jnp.int32, full.shape, 0)
        for h in (2 * pair, 2 * pair + 1):
            own = (row >= KEY_DIM) if h % 2 else (row < KEY_DIM)
            high, low = split(jnp.where(own, full, 0.0))
            enter_ref[0, h] = high
            enter_ref[1, h] = low
    ring.pump_to(PUMP_MIX)

    @pl.loop(0, blocks)
    def _(b):
        mix_block(
            heads, b, q_ref, out_gate_ref, head_gain_ref, top_ref, cum_ref, num_ref, den_ref,
            in_top, enter_ref, mixed_ref,
        )

    tile = 512 if width % 512 == 0 else width

    def product(chunk, piece, store):
        start = pl.multiple_of(chunk * rows + piece * step, step)
        left = mixed_ref[pl.ds(start, step), :]

        @pl.loop(0, width // tile)
        def _(j):
            cols = pl.ds(pl.multiple_of(j * tile, tile), tile)
            store(cols, mm(left, out_weight_ref[:, cols]))

    sent, landing = [], []
    done = 0
    for k in list(range(1, xs)) + [0]:
        to_x = lax.rem(at_x + k, xs)
        for s in range(pieces):
            span = pl.ds(s * step, step)

            def put_pair(cols, block, k=k, span=span):
                pair_out[k, span, cols] = block.astype(bf16)

            product(to_x * CORES + 1 - core, s, put_pair)
            copy = remote(
                pair_out.at[k, span], pair_in.at[k, span],
                pair_send.at[k, s], pair_recv.at[k, s], {"tp": partner},
            )
            copy.start()
            sent.append(copy)

            def put_own(cols, block, span=span):
                total[span, cols] = block.astype(bf16).astype(f32)

            product(to_x * CORES + core, s, put_own)
            copy.wait_recv()
            summed = total[span, :] + pair_in[k, span, :].astype(f32)
            if k == 0:
                total[span, :] = summed
            else:
                x_out[k - 1, span, :] = summed.astype(bf16)
                copy = remote(
                    x_out.at[k - 1, span], x_in.at[k - 1, span],
                    x_send.at[k, s], x_recv.at[k, s], {"tp": peers[k]},
                )
                copy.start()
                sent.append(copy)
                landing.append((s, copy))
    ring.pump_to(PUMP_REDUCED)

    def block(device, s):
        start = pl.multiple_of(HALO + device * rows + s * step, HALO)
        return normed_ref.at[pl.ds(start, step)]

    for s in range(pieces):
        span = pl.ds(s * step, step)
        for at, copy in landing:
            if at == s:
                copy.wait_recv()
        summed = total[span, :]
        for k in range(1, xs):
            summed = summed + x_in[k - 1, span, :].astype(f32)
        mixer_out = summed.astype(bf16).astype(f32)
        after = residual_ref[span, :].astype(f32) + rms_gain(mixer_out, cell_gain_ref[...])
        after = after.astype(bf16)
        after_ref[span, :] = after
        normed = rms_gain(after.astype(f32), ffn_gain_ref[...])
        start = pl.multiple_of(HALO + me * rows + s * step, HALO)
        normed_ref[pl.ds(start, step), :] = normed.astype(bf16)
        own = block(me, s)
        for k in range(1, xs):
            sent.append(remote(own, own, gx_send.at[k, s], gx_recv.at[k, s], {"tp": peers[k]}))
            sent[-1].start()
        sent.append(remote(own, own, gp_send.at[0, s], gp_recv.at[0, s], {"tp": partner}))
        sent[-1].start()
        ring.pump_to(PUMP_NORM[s])
    for s in range(pieces):
        for k in range(1, xs):
            came = block(sources[k], s)
            remote(came, came, gx_send.at[k, s], gx_recv.at[k, s], {"tp": peers[k]}).wait_recv()
            sent.append(remote(came, came, gp_send.at[k, s], gp_recv.at[k, s], {"tp": partner}))
            sent[-1].start()
        ring.pump_to(PUMP_GATHER[s])
    for s in range(pieces):
        for k in range(xs):
            came = block(sources[k] + partner - me, s)
            remote(came, came, gp_send.at[k, s], gp_recv.at[k, s], {"tp": partner}).wait_recv()

    ahead, behind = lax.rem(sp + 1, sps), lax.rem(sp + sps - 1, sps)
    tail = normed_ref.at[pl.ds(tok_rows, HALO)]
    head = normed_ref.at[pl.ds(0, HALO)]

    @pl.when(sp + 1 < sps)
    def _():
        remote(tail, head, h_sems.at[0], h_sems.at[1], {"sp": ahead}).start()

    @pl.when(sp == 0)
    def _():
        normed_ref[pl.ds(0, HALO), :] = jnp.zeros((HALO, width), bf16)

    ring.pump_to(PUMP_UP)
    own_up.wait()
    ring.arrived_all("up")

    @pl.when(sp > 0)
    def _():
        remote(tail, head, h_sems.at[0], h_sems.at[1], {"sp": behind}).wait_recv()

    tiles, half = up_own.shape[0], up_own.shape[2] // 2

    def up_tile(j, cols):
        lift_ref[...] = mm(normed_ref[...], up_all[j]).astype(bf16).astype(f32)
        sums = []
        for taps, side in ((gate_taps_ref, 0), (value_taps_ref, 1)):
            summed = jnp.zeros((tok_rows, half), f32)
            for offset in range(WIDTH):
                tap = taps[offset : offset + 1, cols].astype(f32)
                at = pl.ds(HALO - WIDTH + 1 + offset, tok_rows)
                summed = summed + tap * lift_ref[at, pl.ds(side * half, half)]
            sums.append(summed)
        active_ref[:, cols] = (jax.nn.gelu(sums[0], approximate=True) * sums[1]).astype(bf16)

    if half % LANES == 0:
        edges = [tiles * i // len(PUMP_TILES) for i in range(len(PUMP_TILES) + 1)]
        for i, number in enumerate(PUMP_TILES):

            @pl.loop(edges[i], edges[i + 1])
            def _(j):
                up_tile(j, pl.ds(pl.multiple_of(j * half, half), half))

            ring.pump_to(number)
    else:
        for j in range(tiles):
            up_tile(j, pl.ds(j * half, half))

    own_down.wait()

    def close_columns(shard, slot):
        copies = []
        weight = down_all[shard]
        order = list(range(1, xs)) + [0]
        for k in order:
            chunk = lax.rem(at_x + k, xs) * CORES + 1 - core
            left = active_ref[pl.ds(pl.multiple_of(chunk * rows, rows), rows), :]
            pair_out2[shard, k] = mm(left, weight).astype(bf16)
            copy = remote(
                pair_out2.at[shard, k], pair_in2.at[shard, k],
                p2_send.at[slot, k], p2_recv.at[slot, k], {"tp": partner},
            )
            copy.start()
            copies.append(copy)
        for at, k in enumerate(order):
            chunk = lax.rem(at_x + k, xs) * CORES + core
            left = active_ref[pl.ds(pl.multiple_of(chunk * rows, rows), rows), :]
            part = mm(left, weight).astype(bf16).astype(f32)
            copies[at].wait_recv()
            summed = part + pair_in2[shard, k].astype(f32)
            if k == 0:
                total2[shard] = summed
            else:
                x_out2[shard, k - 1] = summed.astype(bf16)
                copy = remote(
                    x_out2.at[shard, k - 1], x_in2.at[shard, k - 1],
                    x2_send.at[slot, k], x2_recv.at[slot, k], {"tp": peers[k]},
                )
                copy.start()
                final.append(copy)
        sent.extend(copies)

    final = []
    close_columns(sp, 0)
    slot = 1
    for hop in range(1, sps // 2 + 1):
        for way in range(2):
            if hop == sps // 2 and way == 1:
                continue
            for event in ring.events[way]:
                if event[0] == "down" and event[3] == hop:
                    ring.arrived(way, event)
            if hop == sps // 2:
                for event in ring.events[1]:
                    if event[0] == "down" and event[3] == hop:
                        ring.arrived(1, event)
            if way == 0 or hop == sps // 2:
                ring.pump(1)
            close_columns(ring.shard(way, hop), slot)
            slot += 1
            ring.pump(1)
    ring.pump(len(ring.events[0]))
    for copy in final:
        copy.wait_recv()
    square = jnp.zeros((rows, 1), f32)
    for n in range(sps):
        summed = total2[n]
        for k in range(1, xs):
            summed = summed + x_in2[n, k - 1].astype(f32)
        summed = summed.astype(bf16).astype(f32)
        total2[n] = summed
        square = square + jnp.sum(summed * summed, axis=-1, keepdims=True)
    scale = rms_scale(square, width)
    part = width // sps
    for n in range(sps):
        cols = slice(n * part, (n + 1) * part)
        result = after_ref[:, cols].astype(f32) + total2[n] * scale * close_gain_ref[:, cols]
        out_ref[:, cols] = result.astype(bf16)
    for copy in sent + final + ring.sent:
        copy.wait_send()
    for d in range(1, sps):

        @pl.when(sp + d < sps)
        def _(d=d):
            ahead = {"sp": lax.rem(sp + d, sps)}
            remote(small_out, small_in.at[d], t_send.at[d], t_recv.at[d], ahead).wait_send()
            remote(cells_out, cells_in.at[d], s_send.at[d], s_recv.at[d], ahead).wait_send()

    @pl.when(sp + 1 < sps)
    def _():
        remote(tail, head, h_sems.at[0], h_sems.at[1], {"sp": ahead}).wait_send()


PUMP_START = 4
PUMP_STATE = 5
PUMP_MIX = 7
PUMP_REDUCED = 9
PUMP_NORM = (10, 10)
PUMP_GATHER = (11, 12)
PUMP_UP = 16
PUMP_TILES = (16, 17, 18, 19)


def ring_shards(
    queries,
    keys,
    values,
    output_gate_logits,
    log_input_gate,
    forget_gate_logits,
    extra_forget_terms,
    per_head_norm_gain,
    output_weight,
    residual,
    after_cell_norm_gain,
    feedforward_norm_gain,
    closing_norm_gain,
    gate_up_weight,
    value_up_weight,
    gate_filter_taps,
    value_filter_taps,
    down_weight,
):
    count, sps = lax.axis_size("tp"), lax.axis_size("sp")
    xs = count // CORES
    tok_rows = queries.shape[0]
    heads = log_input_gate.shape[0]
    own_depth, hidden = gate_up_weight.shape
    width = output_weight.shape[1]
    own_width = down_weight.shape[1]
    rows = tok_rows // count
    pieces = 2
    half = LANES if hidden % LANES == 0 else LANES // 2
    tiles = hidden // half
    up_own = jnp.concatenate(
        [
            gate_up_weight.reshape(own_depth, tiles, half),
            value_up_weight.reshape(own_depth, tiles, half),
        ],
        axis=2,
    ).transpose(1, 0, 2)
    events = len(ring_events(sps)[0])
    vmem = pl.BlockSpec(memory_space=pltpu.VMEM)
    hbm = pl.BlockSpec(memory_space=pl.ANY)
    dma = pltpu.SemaphoreType.DMA
    V = pltpu.VMEM
    small = -(-(heads // 2 + 2 * heads) // 8) * 8
    pairs = heads // 2
    return pl.pallas_call(
        functools.partial(step_kernel, count, sps, pieces),
        out_shape=jax.ShapeDtypeStruct(residual.shape, bf16),
        in_specs=[vmem] * 13 + [hbm, vmem, vmem, hbm],
        out_specs=vmem,
        scratch_shapes=[
            V((tiles, own_depth * sps, 2 * half), bf16),
            V((sps, hidden, own_width), bf16),
            V((8, tok_rows), f32),
            V((8, tok_rows), f32),
            V((8, tok_rows), f32),
            V((tok_rows, heads * VAL_DIM), f32),
            V((tok_rows, heads * VAL_DIM), f32),
            V((heads, LANES, 2 * LANES), f32),
            V((8, LANES), f32),
            V((pairs, LANES, LANES), f32),
            V((small, LANES), f32),
            V((sps, pairs, LANES, LANES), f32),
            V((sps, small, LANES), f32),
            V((pairs, LANES, LANES), f32),
            V((8, LANES), f32),
            V((8, LANES), f32),
            V((8, LANES), f32),
            V((2, heads, LANES, 2 * LANES), bf16),
            V((tok_rows, heads * VAL_DIM), bf16),
            V((rows, width), f32),
            V((xs, rows, width), bf16),
            V((xs, rows, width), bf16),
            V((max(xs - 1, 1), rows, width), bf16),
            V((max(xs - 1, 1), rows, width), bf16),
            V((rows, width), bf16),
            V((HALO + tok_rows, width), bf16),
            V((HALO + tok_rows, 2 * half), f32),
            V((tok_rows, hidden), bf16),
            V((sps, rows, own_width), f32),
            V((sps, xs, rows, own_width), bf16),
            V((sps, xs, rows, own_width), bf16),
            V((sps, max(xs - 1, 1), rows, own_width), bf16),
            V((sps, max(xs - 1, 1), rows, own_width), bf16),
            dma((2, events)),
            dma((2, events)),
            dma((2,)),
            dma((sps,)),
            dma((sps,)),
            dma((sps,)),
            dma((sps,)),
            dma((2,)),
        ]
        + [dma((xs, pieces))] * 8
        + [dma((sps, xs))] * 4,
        compiler_params=pltpu.CompilerParams(
            collective_id=0, has_side_effects=True, vmem_limit_bytes=VMEM_BYTES
        ),
        cost_estimate=pl.CostEstimate(
            flops=6 * tok_rows * hidden * width, bytes_accessed=3 * 10**7, transcendentals=0
        ),
        name="step",
    )(
        queries, keys, values, output_gate_logits, log_input_gate, forget_gate_logits,
        extra_forget_terms, per_head_norm_gain.reshape(1, -1), output_weight, residual,
        after_cell_norm_gain.reshape(1, -1), feedforward_norm_gain.reshape(1, -1),
        closing_norm_gain.reshape(1, -1), up_own, gate_filter_taps, value_filter_taps, down_weight,
    )


class Line:
    def __init__(self, rows_z, up_own, up_all, down_own, down_all, y_send, y_recv, send, recv):
        self.rows_z = rows_z
        self.up_own, self.up_all = up_own, up_all
        self.down_own, self.down_all = down_own, down_all
        self.y_send, self.y_recv, self.send, self.recv = y_send, y_recv, send, recv
        self.sp = lax.axis_index("sp")
        self.z, self.y = self.sp // 2, lax.rem(self.sp, 2)
        self.units = [("main", yy, r) for yy in range(2) for r in range(2)]
        self.units += [("edge", yy, 0) for yy in range(2)] + [("down", yy, 0) for yy in range(2)]
        last = rows_z - 1
        order = [("main", hop) for hop in range(1, last)] + [("edge", 1), ("main", last)]
        order += [("edge", hop) for hop in range(2, last + 1)]
        order += [("down", hop) for hop in range(1, last + 1)]
        if last == 1:
            order = [("main", 1), ("edge", 1), ("down", 1)]
        self.events = [
            (unit, hop) for kind, hop in order for unit in self.units if unit[0] == kind
        ]
        self.waited = set()
        self.next = 0

    def piece(self, unit, z, y):
        kind, _, r = unit
        shard = z * 2 + y
        if kind == "down":
            return self.down_all.at[shard]
        rows = self.up_own.shape[1]
        if kind == "edge":
            return self.up_all.at[pl.ds(pl.multiple_of(shard * rows, rows), rows), self.cols(kind)]
        start = pl.multiple_of(shard * rows + r * (rows // 2), rows // 2)
        return self.up_all.at[pl.ds(start, rows // 2), self.cols(kind)]

    def cols(self, kind):
        width = self.up_all.shape[1]
        main = main_tiles(width // 2) * 2 * LANES
        return pl.ds(0, main) if kind == "main" else pl.ds(main, width - main)

    def own(self, unit, y):
        kind, _, r = unit
        if kind == "down":
            rows = self.down_all.shape[1]
            return self.down_own.at[pl.ds(pl.multiple_of(y * rows, rows), rows)]
        rows = self.up_own.shape[1]
        if kind == "edge":
            return self.up_own.at[y, :, self.cols(kind)]
        return self.up_own.at[y, pl.ds(r * (rows // 2), rows // 2), self.cols(kind)]

    def side(self, yy):
        return self.y if yy == 0 else 1 - self.y

    def across(self, unit):
        at = self.units.index((unit[0], 1, unit[2]))
        return remote(
            self.own(unit, 1 - self.y), self.piece(unit, self.z, self.y),
            self.y_send.at[at], self.y_recv.at[at], {"sp": self.z * 2 + 1 - self.y},
        )

    def start_across(self, *kinds):
        for unit in self.units:
            if unit[1] == 1 and unit[0] in kinds:
                self.across(unit).start()

    def came_across(self, unit):
        if unit in self.waited:
            return
        self.waited.add(unit)
        at = self.units.index(unit)
        came = self.piece(unit, self.z, 1 - self.y)
        remote(
            came, came, self.y_send.at[at], self.y_recv.at[at], {"sp": self.z * 2 + 1 - self.y}
        ).wait_recv()

    def valid(self, way, hop):
        return self.z - hop >= 0 if way == 0 else self.z + hop < self.rows_z

    def origin(self, way, hop):
        return self.z - hop if way == 0 else self.z + hop

    def onward(self, way):
        return lax.rem(self.z + (1 if way == 0 else self.rows_z - 1), self.rows_z)

    def sends(self, way, hop):
        onward = self.z + 1 < self.rows_z if way == 0 else self.z >= 1
        return jnp.logical_and(onward, self.valid(way, hop - 1))

    def copy(self, way, event):
        unit, hop = event
        at = self.events.index(event)
        y = self.side(unit[1])
        dst = self.piece(unit, self.origin(way, hop - 1), y)
        src = self.own(unit, self.y) if hop == 1 and unit[1] == 0 else dst
        target = {"sp": self.onward(way) * 2 + self.y}
        return remote(src, dst, self.send.at[way, at], self.recv.at[way, at], target)

    def arrived(self, way, event):
        if (way, event) in self.waited:
            return
        self.waited.add((way, event))
        unit, hop = event
        at = self.events.index(event)

        @pl.when(self.valid(way, hop))
        def _():
            came = self.piece(unit, self.origin(way, hop), self.side(unit[1]))
            where = {"sp": self.onward(1 - way) * 2 + self.y}
            remote(came, came, self.send.at[way, at], self.recv.at[way, at], where).wait_recv()

    def pump_to(self, number):
        while self.next < min(number, len(self.events)):
            event = self.events[self.next]
            unit, hop = event
            if hop == 1 and unit[1] == 1:
                self.came_across(unit)
            for way in range(2):
                if hop > 1:
                    self.arrived(way, (unit, hop - 1))
                sends = self.sends(way, hop)
                if unit[0] == "down" and hop == 1:
                    sends = jnp.logical_and(sends, self.sends(way, self.rows_z - 1))

                @pl.when(sends)
                def _(way=way, event=event):
                    self.copy(way, event).start()

            self.next += 1

    def start_down(self):
        for event in self.events:
            unit, hop = event
            if unit[0] == "down" and hop == 1:
                if unit[1] == 1:
                    self.came_across(unit)
                for way in range(2):
                    last = self.sends(way, self.rows_z - 1)

                    @pl.when(jnp.logical_and(self.sends(way, 1), jnp.logical_not(last)))
                    def _(way=way, event=event):
                        self.copy(way, event).start()

    def arrived_all(self, kind):
        for unit in self.units:
            if unit[0] == kind and unit[1] == 1:
                self.came_across(unit)
        for event in self.events:
            if event[0][0] == kind:
                for way in range(2):
                    self.arrived(way, event)

    def wait_sends(self):
        for unit in self.units:
            if unit[1] == 1:
                self.across(unit).wait_send()
        for event in self.events:
            for way in range(2):

                @pl.when(self.sends(way, event[1]))
                def _(way=way, event=event):
                    self.copy(way, event).wait_send()


def main_tiles(hidden):
    return max(hidden // LANES - 1, 1)


def whole_state(heads, blocks, k_ref, v_ref, reach_ref, top_ref, state_ref, held_ref):
    last = top_ref[:, pl.ds(blocks * CHUNK - LANES, LANES)]
    now = jnp.broadcast_to(last[:, LANES - 1 :], last.shape)
    held_ref[...] = now
    state_ref[...] = jnp.zeros_like(state_ref)
    ones = jnp.ones((CHUNK, LANES), bf16)
    at_k = lax.broadcasted_iota(jnp.int32, (CHUNK, CHUNK), 0)

    @pl.loop(0, blocks)
    def _(b):
        rows = pl.ds(pl.multiple_of(b * CHUNK, CHUNK), CHUNK)
        weight = jnp.exp(reach_ref[:, rows] - now)
        for pair in range(heads // 2):
            turned_keys = k_ref[rows, pl.ds(pair * LANES, LANES)].astype(f32).T
            for h in (2 * pair, 2 * pair + 1):
                value = jnp.concatenate([v_ref[rows, pl.ds(h * VAL_DIM, VAL_DIM)], ones], axis=1)
                own = (at_k >= KEY_DIM) if h % 2 else (at_k < KEY_DIM)
                high, low = split(jnp.where(own, turned_keys, 0.0) * weight[h : h + 1, :])
                state_ref[h] += mm(high, value) + mm(low, value)


def clear_state(in_cells, in_norm, in_top, in_after):
    in_cells[...] = jnp.zeros_like(in_cells)
    in_norm[...] = jnp.zeros_like(in_norm)
    in_top[...] = jnp.full_like(in_top, empty_log)
    in_after[...] = jnp.zeros_like(in_after)


def total_square(array):
    return jnp.sum(jnp.sum(array * array, axis=2, keepdims=True), axis=0, keepdims=True)


def plane_kernel(
    count, sps, pieces,
    q_ref, k_ref, v_ref, out_gate_ref, in_gate_ref, forget_ref, extra_ref, head_gain_ref,
    out_weight_ref, residual_ref, cell_gain_ref, ffn_gain_ref, close_gain_ref,
    gate_up_ref, value_up_ref, gate_taps_ref, value_taps_ref, down_own,
    out_ref,
    up_own, taps_ref, up_all, down_all,
    reach_ref, top_ref, cum_ref, num_ref, den_ref, state_ref, held_ref,
    y_cells, y_small, z_cells, z_small, p_cells, p_small,
    in_cells, in_norm, in_top, in_after, enter_ref,
    mixed_ref, total, pair_out, pair_in, one_out, one_in, two_out, two_in,
    after_ref, normed_ref, lift_ref, active_ref,
    wy_send, wy_recv, wz_send, wz_recv, own_sems,
    sy_send, sy_recv, sz_send, sz_recv, h_sems,
    pair_send, pair_recv, x_send, x_recv,
    ax_send, ax_recv, ay_send, ay_recv, ad_send, ad_recv, gp_send, gp_recv,
    p2_send, p2_recv, one_send, one_recv, two_send, two_recv,
):
    sp = lax.axis_index("sp")
    me = lax.axis_index("tp")
    z, y = sp // 2, lax.rem(sp, 2)
    x, core = me // CORES, lax.rem(me, CORES)
    rows_z = sps // 2
    partner, x_peer = {"tp": x * CORES + 1 - core}, {"tp": (1 - x) * CORES + core}
    y_peer = {"sp": z * 2 + 1 - y}
    tok_rows, heads = q_ref.shape[0], in_gate_ref.shape[0]
    blocks = tok_rows // CHUNK
    rows = tok_rows // count
    step = rows // pieces
    width = out_weight_ref.shape[1]
    cw = width // sps
    pairs = heads // 2
    line = Line(
        rows_z, up_own, up_all, down_own, down_all, wy_send, wy_recv, wz_send, wz_recv
    )

    barrier = pltpu.get_barrier_semaphore()
    friends = [partner, x_peer, y_peer]
    friends += [{"sp": lax.rem(z + d, rows_z) * 2 + y} for d in range(1, rows_z)]
    for where in friends:
        pl.semaphore_signal(barrier, inc=1, device_id=where, device_id_type=MESH)
    hidden = active_ref.shape[1]
    for side in range(2):
        for start in range(0, hidden, LANES):
            size = min(LANES, hidden - start)
            for at, weight in ((0, gate_up_ref), (size, value_up_ref)):
                up_own[side, :, 2 * start + at : 2 * start + at + size] = weight[
                    :, side * hidden + start : side * hidden + start + size
                ]
    for at, taps in enumerate((gate_taps_ref, value_taps_ref)):
        both = taps[...].astype(f32)
        taps_ref[at, 0:WIDTH, :] = jnp.where(y == 0, both[:, :hidden], both[:, hidden:])
    pl.semaphore_wait(barrier, len(friends))

    line.start_across("main")
    line.pump_to(LINE_START)
    own_rows = up_own.shape[1]
    own_up = pltpu.make_async_copy(
        up_own.at[y],
        up_all.at[pl.ds(pl.multiple_of(sp * own_rows, own_rows), own_rows)],
        own_sems.at[0],
    )
    own_up.start()
    own_down = pltpu.make_async_copy(
        line.own(("down", 0, 0), y), down_all.at[sp], own_sems.at[1]
    )
    own_down.start()

    gate_rows_into(heads, in_gate_ref, forget_ref, extra_ref, reach_ref, top_ref, cum_ref)
    whole_state(heads, blocks, k_ref, v_ref, reach_ref, top_ref, state_ref, held_ref)
    last = cum_ref[:, pl.ds(tok_rows - LANES, LANES)]
    cum_last = jnp.broadcast_to(last[:, LANES - 1 :], last.shape)
    pack_state(heads, state_ref, held_ref, cum_last, y_cells.at[y], y_small.at[y])

    def swap(array, side, at):
        return remote(array.at[side], array.at[side], sy_send.at[at], sy_recv.at[at], y_peer)

    swap(y_small, y, 0).start()
    swap(y_cells, y, 1).start()
    line.start_across("edge", "down")
    line.pump_to(LINE_SWAP)
    state_ref[...] = jnp.zeros_like(state_ref)
    held_ref[...] = jnp.full_like(held_ref, empty_log)

    def cell_blocks(low, high):
        @pl.loop(low, high)
        def _(b):
            cell_block(
                heads, b, q_ref, k_ref, v_ref, reach_ref, top_ref, num_ref, den_ref,
                state_ref, held_ref,
            )

    cell_blocks(0, blocks * CELL_SPLIT // 8)
    swap(y_small, 1 - y, 0).wait_recv()
    swap(y_cells, 1 - y, 1).wait_recv()
    acc = (in_cells, in_norm, in_top, in_after)
    clear_state(*acc)
    merge_state(heads, y_cells.at[1], y_small.at[1], *acc)
    merge_state(heads, y_cells.at[0], y_small.at[0], *acc)
    p_cells[...] = in_cells[...]
    p_small[...] = jnp.concatenate(
        [
            in_norm[0:pairs, :], in_top[0:heads, :], in_after[0:heads, :],
            jnp.zeros((p_small.shape[0] - pairs - 2 * heads, LANES), f32),
        ],
        axis=0,
    )

    def along(d):
        where = {"sp": lax.rem(z + d, rows_z) * 2 + y}
        return (
            remote(p_small, z_small.at[d], sz_send.at[0, d], sz_recv.at[0, d], where),
            remote(p_cells, z_cells.at[d], sz_send.at[1, d], sz_recv.at[1, d], where),
        )

    for d in range(1, rows_z):

        @pl.when(z + d < rows_z)
        def _(d=d):
            for copy in along(d):
                copy.start()

    line.pump_to(LINE_STATE[0])
    cell_blocks(blocks * CELL_SPLIT // 8, blocks)
    line.pump_to(LINE_STATE[1])
    clear_state(*acc)

    @pl.when(y == 1)
    def _():
        merge_state(heads, y_cells.at[0], y_small.at[0], *acc)

    for d in range(1, rows_z):

        @pl.when(z - d >= 0)
        def _(d=d):
            for copy in along(d):
                copy.wait_recv()
            merge_state(heads, z_cells.at[d], z_small.at[d], *acc)

    for pair in range(pairs):
        norm = jnp.broadcast_to(in_norm[pair : pair + 1, :], (LANES, LANES)).T
        full = jnp.concatenate([in_cells[pair], norm], axis=1)
        row = lax.broadcasted_iota(jnp.int32, full.shape, 0)
        for h in (2 * pair, 2 * pair + 1):
            own = (row >= KEY_DIM) if h % 2 else (row < KEY_DIM)
            high, low = split(jnp.where(own, full, 0.0))
            enter_ref[0, h] = high
            enter_ref[1, h] = low
    line.pump_to(LINE_MIX)

    def mix_blocks(at_x):
        @pl.loop(0, blocks // 2)
        def _(b):
            mix_block(
                heads, at_x * (blocks // 2) + b, q_ref, out_gate_ref, head_gain_ref, top_ref,
                cum_ref, num_ref, den_ref, in_top, enter_ref, mixed_ref,
            )

    def product(chunk, piece, store):
        start = pl.multiple_of(chunk * rows + piece * step, step)
        left = mixed_ref[pl.ds(start, step), :]

        @pl.loop(0, sps)
        def _(j):
            cols = pl.ds(pl.multiple_of(j * cw, cw), cw)
            store(j, mm(left, out_weight_ref[:, cols]))

    sent, landing = [], []
    for k in (1, 0):
        to_x = x if k == 0 else 1 - x
        mix_blocks(to_x)
        for s in range(pieces):
            span = pl.ds(s * step, step)

            def put_pair(j, block, k=k, span=span):
                pair_out[j, k, span, :] = block.astype(bf16)

            product(to_x * CORES + 1 - core, s, put_pair)
            copy = remote(
                pair_out.at[:, k, span], pair_in.at[:, k, span],
                pair_send.at[k, s], pair_recv.at[k, s], partner,
            )
            copy.start()
            sent.append(copy)

            def put_own(j, block, span=span):
                total[j, span, :] = block.astype(bf16).astype(f32)

            product(to_x * CORES + core, s, put_own)
            copy.wait_recv()
            summed = total[:, span, :] + pair_in[:, k, span, :].astype(f32)
            if k == 0:
                total[:, span, :] = summed
            else:
                one_out[:, s] = summed.astype(bf16)
                copy = remote(
                    one_out.at[:, s], one_in.at[:, s], x_send.at[s], x_recv.at[s], x_peer
                )
                copy.start()
                sent.append(copy)
                landing.append(copy)
        line.pump_to(LINE_REDUCED[1 - k])

    def block(side, owner, s):
        start = pl.multiple_of(HALO + side * tok_rows + owner * rows + s * step, HALO)
        return normed_ref.at[pl.ds(start, step)]

    def give(array, sems, at, where):
        copy = remote(array, array, sems[0].at[at], sems[1].at[at], where)
        copy.start()
        sent.append(copy)

    def take(array, sems, at, where):
        remote(array, array, sems[0].at[at], sems[1].at[at], where).wait_recv()

    to_x, to_y, to_d = (ax_send, ax_recv), (ay_send, ay_recv), (ad_send, ad_recv)
    to_p = (gp_send, gp_recv)
    other = (1 - x) * CORES + core
    for s in range(pieces):
        span = pl.ds(s * step, step)
        landing[s].wait_recv()
        summed = total[:, span, :] + one_in[:, s].astype(f32)
        mixer_out = summed.astype(bf16).astype(f32)
        scale = rms_scale(total_square(mixer_out), width)
        held = []
        for j in range(sps):
            cols = slice(j * cw, (j + 1) * cw)
            after = residual_ref[span, cols].astype(f32) + (
                mixer_out[j] * scale[0] * cell_gain_ref[:, cols]
            )
            after = after.astype(bf16)
            after_ref[j, span, :] = after
            held.append(after.astype(f32))
        square = sum(jnp.sum(a * a, axis=-1, keepdims=True) for a in held)
        scale = rms_scale(square, width)
        start = pl.multiple_of(HALO + y * tok_rows + me * rows + s * step, HALO)
        for j in range(sps):
            cols = slice(j * cw, (j + 1) * cw)
            normed_ref[pl.ds(start, step), cols] = (
                held[j] * scale * ffn_gain_ref[:, cols]
            ).astype(bf16)
        own = block(y, me, s)
        give(own, to_y, s, y_peer)
        give(own, to_x, s, x_peer)
        give(own, to_p, s, partner)
        line.pump_to(LINE_NORM[s])
    for s in range(pieces):
        from_x, from_y = block(y, other, s), block(1 - y, me, s)
        if s == 0:
            take(from_y, to_y, s, y_peer)
            give(from_y, to_d, s, x_peer)
            give(from_y, to_p, 2 * pieces + s, partner)
            take(from_x, to_x, s, x_peer)
            give(from_x, to_p, pieces + s, partner)
        else:
            take(from_x, to_x, s, x_peer)
            give(from_x, to_d, s, y_peer)
            give(from_x, to_p, pieces + s, partner)
            take(from_y, to_y, s, y_peer)
            give(from_y, to_p, 2 * pieces + s, partner)
        line.pump_to(LINE_GATHER[s])
    for s in range(pieces):
        from_d = block(1 - y, other, s)
        take(from_d, to_d, s, x_peer if s == 0 else y_peer)
        give(from_d, to_p, 3 * pieces + s, partner)
        line.pump_to(LINE_DIAGONAL[s])
    mate, other_mate = x * CORES + 1 - core, (1 - x) * CORES + 1 - core
    for s in range(pieces):
        take(block(y, mate, s), to_p, s, partner)
        take(block(y, other_mate, s), to_p, pieces + s, partner)
        take(block(1 - y, mate, s), to_p, 2 * pieces + s, partner)
        take(block(1 - y, other_mate, s), to_p, 3 * pieces + s, partner)

    group = 2 * tok_rows

    def halo(plane):
        return remote(
            normed_ref.at[pl.ds(group, HALO)], normed_ref.at[pl.ds(0, HALO)],
            h_sems.at[0], h_sems.at[1], {"sp": lax.rem(plane, rows_z) * 2 + y},
        )

    @pl.when(z + 1 < rows_z)
    def _():
        halo(z + 1).start()

    @pl.when(z == 0)
    def _():
        normed_ref[pl.ds(0, HALO), :] = jnp.zeros((HALO, width), bf16)

    line.start_down()
    line.pump_to(LINE_UP)
    own_up.wait()
    line.arrived_all("main")

    @pl.when(z > 0)
    def _():
        halo(z + rows_z - 1).wait_recv()

    full, rest = hidden // LANES, hidden % LANES

    def up_tile(weight_cols, cols, half):
        lift_ref[:, pl.ds(0, 2 * half)] = (
            mm(normed_ref[...], up_all[:, weight_cols]).astype(bf16).astype(f32)
        )

        @pl.loop(0, group // CONV_ROWS)
        def _(i):
            sums = []
            for side in range(2):
                summed = jnp.zeros((CONV_ROWS, half), f32)
                base = pl.multiple_of(i * CONV_ROWS, CONV_ROWS)
                window = lift_ref[pl.ds(base, CONV_ROWS + HALO), pl.ds(side * half, half)]
                for offset in range(WIDTH):
                    tap = taps_ref[side, offset : offset + 1, cols]
                    low = HALO - WIDTH + 1 + offset
                    summed = summed + tap * window[low : low + CONV_ROWS]
                sums.append(summed)
            active = jax.nn.gelu(sums[0], approximate=True) * sums[1]
            active_ref[pl.ds(base, CONV_ROWS), cols] = active.astype(bf16)

    def up_tiles(low, high):
        @pl.loop(low, high)
        def _(j):
            up_tile(
                pl.ds(pl.multiple_of(j * 2 * LANES, 2 * LANES), 2 * LANES),
                pl.ds(pl.multiple_of(j * LANES, LANES), LANES),
                LANES,
            )

    main = main_tiles(hidden)
    up_tiles(0, main // 2)
    line.pump_to(LINE_TILES[0])
    up_tiles(main // 2, main)
    line.pump_to(LINE_TILES[1])
    line.arrived_all("edge")
    up_tiles(main, full)
    if rest:
        up_tile(pl.ds(full * 2 * LANES, 2 * rest), pl.ds(full * LANES, rest), rest)
    line.pump_to(LINE_TILES[2])

    own_down.wait()
    for copy in sent:
        copy.wait_send()

    def chunk_rows(side, at_x, at_core):
        start = side * tok_rows + (at_x * CORES + at_core) * rows
        return pl.ds(pl.multiple_of(start, rows), rows)

    def pair_copy(shard, k):
        return remote(
            pair_out.at[shard, k], pair_in.at[shard, k],
            p2_send.at[shard, k], p2_recv.at[shard, k], partner,
        )

    def one_copy(shard, at, where=None):
        where = where or (x_peer if at < 2 else y_peer)
        return remote(
            one_out.at[shard, at], one_in.at[shard, at],
            one_send.at[shard, at], one_recv.at[shard, at], where,
        )

    def two_copy(shard, at):
        return remote(
            two_out.at[shard, at], two_in.at[shard, at],
            two_send.at[shard, at], two_recv.at[shard, at], y_peer if at == 0 else x_peer,
        )

    low, high = pl.ds(0, step), pl.ds(step, rows - step)

    def side_of(k):
        return jnp.where(lax.rem(k, 2) == 0, 1 - y, y), jnp.where(k < 2, 1 - x, x)

    def part_rows(k, start, size):
        return pl.ds(pl.multiple_of(k * rows + start, step), size)

    def multiply(shard):
        weight = down_all.at[shard]

        @pl.loop(0, 4)
        def _(k):
            left = active_ref[chunk_rows(*side_of(k), 1 - core), :]
            pair_out[shard, k] = mm(left, weight[...]).astype(bf16)
            pair_copy(shard, k).start()

        @pl.loop(0, 4)
        def _(k):
            left = active_ref[chunk_rows(*side_of(k), core), :]
            part = mm(left, weight[...]).astype(bf16).astype(f32)
            pair_copy(shard, k).wait_recv()
            lift_ref[part_rows(k, 0, rows), :] = part + pair_in[shard, k].astype(f32)

            @pl.when(k < 2)
            def _():
                one_out[shard, k] = lift_ref[part_rows(k, 0, step), :].astype(bf16)
                one_copy(shard, k, x_peer).start()

            @pl.when(lax.rem(k, 2) == 0)
            def _():
                at = 2 + k // 2
                one_out[shard, at] = lift_ref[part_rows(k, step, step), :].astype(bf16)
                one_copy(shard, at, y_peer).start()

        two_out[shard, 0] = lift_ref[part_rows(2, 0, step), :].astype(bf16)
        two_out[shard, 1] = lift_ref[part_rows(1, step, step), :].astype(bf16)
        total[shard] = lift_ref[part_rows(3, 0, rows), :]

    def pass_on(shard):
        one_copy(shard, 0).wait_recv()
        summed = two_out[shard, 0].astype(f32) + one_in[shard, 0].astype(f32)
        two_out[shard, 0] = summed.astype(bf16)
        two_copy(shard, 0).start()
        one_copy(shard, 2).wait_recv()
        summed = two_out[shard, 1].astype(f32) + one_in[shard, 2].astype(f32)
        two_out[shard, 1] = summed.astype(bf16)
        two_copy(shard, 1).start()
        one_copy(shard, 1).wait_recv()
        one_copy(shard, 3).wait_recv()

    steps = [(None, 0, 0), (None, 0, 1)]
    for hop in range(1, rows_z):
        for yy in range(2):
            for way in range(2):
                steps.append((way, hop, yy))

    def shard_of(way, hop, yy):
        return (z if way is None else line.origin(way, hop)) * 2 + line.side(yy)

    def at_step(entry, action):
        way, hop, yy = entry
        if way is None:
            action()
        else:
            pl.when(line.valid(way, hop))(action)

    first_down = 6 * (rows_z - 1)
    def finish(shard):
        two_copy(shard, 0).wait_recv()
        two_copy(shard, 1).wait_recv()
        total[shard, low] = (
            total[shard, low] + one_in[shard, 1].astype(f32) + two_in[shard, 0].astype(f32)
        )
        total[shard, high] = (
            total[shard, high] + one_in[shard, 3].astype(f32) + two_in[shard, 1].astype(f32)
        )

    queue = []
    for at in range(len(steps) + LAG_FINISH):
        if at < len(steps):
            way, hop, yy = steps[at]
            unit = ("down", yy, 0)
            if way is None:
                if yy:
                    line.came_across(unit)
            else:
                line.pump_to(first_down + 2 * hop + yy + 1)
                line.arrived(way, (unit, hop))
            queue.append((steps[at], shard_of(*steps[at])))
            entry, shard = queue[at]
            at_step(entry, functools.partial(multiply, shard))
        if 0 <= at - LAG_PASS < len(steps):
            entry, shard = queue[at - LAG_PASS]
            at_step(entry, functools.partial(pass_on, shard))
        if 0 <= at - LAG_FINISH < len(steps):
            entry, shard = queue[at - LAG_FINISH]
            at_step(entry, functools.partial(finish, shard))
    summed = total[...].astype(bf16).astype(f32)
    scale = rms_scale(total_square(summed), width)
    for j in range(sps):
        cols = slice(j * cw, (j + 1) * cw)
        result = after_ref[j].astype(f32) + summed[j] * scale[0] * close_gain_ref[:, cols]
        out_ref[:, cols] = result.astype(bf16)

    for entry in steps:

        def sends_done(entry=entry):
            shard = shard_of(*entry)
            for k in range(4):
                pair_copy(shard, k).wait_send()
                one_copy(shard, k).wait_send()
            for k in range(2):
                two_copy(shard, k).wait_send()

        at_step(entry, sends_done)
    line.wait_sends()
    swap(y_small, y, 0).wait_send()
    swap(y_cells, y, 1).wait_send()
    for d in range(1, rows_z):

        @pl.when(z + d < rows_z)
        def _(d=d):
            for copy in along(d):
                copy.wait_send()

    @pl.when(z + 1 < rows_z)
    def _():
        halo(z + 1).wait_send()


LINE_START = 2
LINE_SWAP = 3
LINE_STATE = (4, 6)
LINE_MIX = 7
LINE_REDUCED = (10, 12)
LINE_NORM = (13, 13)
LINE_GATHER = (14, 15)
LINE_DIAGONAL = (16, 17)
LINE_UP = 20
LINE_TILES = (20, 21, 22)
CELL_SPLIT = 4
LAG_PASS = 4
LAG_FINISH = 14
CONV_ROWS = 256


def plane_shards(
    queries, keys, values, output_gate_logits, log_input_gate, forget_gate_logits,
    extra_forget_terms, per_head_norm_gain, output_weight, residual, after_cell_norm_gain,
    feedforward_norm_gain, closing_norm_gain, gate_up_weight, value_up_weight,
    gate_filter_taps, value_filter_taps, down_weight,
):
    count, sps = lax.axis_size("tp"), lax.axis_size("sp")
    rows_z = sps // 2
    tok_rows = queries.shape[0]
    heads = log_input_gate.shape[0]
    own_depth = gate_up_weight.shape[0]
    hidden = gate_up_weight.shape[1] // 2
    width = output_weight.shape[1]
    cw = down_weight.shape[1]
    rows = tok_rows // count
    pieces = 2
    step = rows // pieces
    vmem = pl.BlockSpec(memory_space=pltpu.VMEM)
    hbm = pl.BlockSpec(memory_space=pl.ANY)
    dma = pltpu.SemaphoreType.DMA
    V = pltpu.VMEM
    pairs = heads // 2
    small = -(-(pairs + 2 * heads) // 8) * 8
    cells = (pairs, LANES, LANES)
    return pl.pallas_call(
        functools.partial(plane_kernel, count, sps, pieces),
        out_shape=jax.ShapeDtypeStruct(residual.shape, bf16),
        in_specs=[vmem] * 17 + [hbm],
        out_specs=vmem,
        scratch_shapes=[
            V((2, own_depth, 2 * hidden), bf16),
            V((2, 8, hidden), f32),
            V((own_depth * sps, 2 * hidden), bf16),
            V((sps, hidden, cw), bf16),
            V((8, tok_rows), f32),
            V((8, tok_rows), f32),
            V((8, tok_rows), f32),
            V((tok_rows, heads * VAL_DIM), f32),
            V((tok_rows, heads * VAL_DIM), f32),
            V((heads, LANES, 2 * LANES), f32),
            V((8, LANES), f32),
            V((2,) + cells, f32),
            V((2, small, LANES), f32),
            V((rows_z,) + cells, f32),
            V((rows_z, small, LANES), f32),
            V(cells, f32),
            V((small, LANES), f32),
            V(cells, f32),
            V((8, LANES), f32),
            V((8, LANES), f32),
            V((8, LANES), f32),
            V((2, heads, LANES, 2 * LANES), bf16),
            V((tok_rows, heads * VAL_DIM), bf16),
            V((sps, rows, cw), f32),
            V((sps, 4, rows, cw), bf16),
            V((sps, 4, rows, cw), bf16),
            V((sps, 4, step, cw), bf16),
            V((sps, 4, step, cw), bf16),
            V((sps, 2, step, cw), bf16),
            V((sps, 2, step, cw), bf16),
            V((sps, rows, cw), bf16),
            V((HALO + 2 * tok_rows, width), bf16),
            V((HALO + 2 * tok_rows, 2 * LANES), f32),
            V((2 * tok_rows, hidden), bf16),
            dma((8,)),
            dma((8,)),
            dma((2, 8 * (rows_z - 1))),
            dma((2, 8 * (rows_z - 1))),
            dma((2,)),
            dma((2,)),
            dma((2,)),
            dma((2, rows_z)),
            dma((2, rows_z)),
            dma((2,)),
            dma((2, pieces)),
            dma((2, pieces)),
            dma((pieces,)),
            dma((pieces,)),
        ]
        + [dma((pieces,))] * 6
        + [dma((4 * pieces,))] * 2
        + [dma((sps, 4))] * 4
        + [dma((sps, 2))] * 2,
        compiler_params=pltpu.CompilerParams(
            collective_id=0, has_side_effects=True, vmem_limit_bytes=VMEM_BYTES
        ),
        cost_estimate=pl.CostEstimate(
            flops=12 * tok_rows * hidden * width, bytes_accessed=3 * 10**7, transcendentals=0
        ),
        name="plane",
    )(
        queries, keys, values, output_gate_logits, log_input_gate, forget_gate_logits,
        extra_forget_terms, per_head_norm_gain.reshape(1, -1), output_weight, residual,
        after_cell_norm_gain.reshape(1, -1), feedforward_norm_gain.reshape(1, -1),
        closing_norm_gain.reshape(1, -1), gate_up_weight, value_up_weight, gate_filter_taps,
        value_filter_taps, down_weight,
    )


def shards(*arrays):
    count, sps = lax.axis_size("tp"), lax.axis_size("sp")
    hidden, own_width = arrays[17].shape
    plane = (
        grid_of(sps)[1] == 2
        and count == 2 * CORES
        and own_width == 2 * LANES
        and hidden % 32 == 0
        and hidden >= 4 * LANES
        and arrays[0].shape[0] % (2 * CHUNK) == 0
    )
    return plane_shards(*arrays) if plane else ring_shards(*arrays)


def solution(mesh):
    placed = (
        P("sp", "tp"),
        P("sp", "tp"),
        P("sp", "tp"),
        P("sp", "tp"),
        P("tp", "sp"),
        P("tp", "sp"),
        P("tp", "sp"),
        P("tp"),
        P("tp", None),
        P(("sp", "tp"), None),
        P(),
        P(),
        P(),
        P("sp", "tp"),
        P("sp", "tp"),
        P(None, "tp"),
        P(None, "tp"),
        P("tp", "sp"),
    )
    return jax.shard_map(
        shards, mesh=mesh, in_specs=placed, out_specs=P(("sp", "tp"), None), check_vma=False
    )
```
